512 devices in a mesh: sp: 64 (over z, y), tp: 8 (over x, core).
Axes of the slice: x: 4, y: 8, z: 8, core: 2. Of those that a mesh axis runs over, the one named last changes fastest.
Arguments:
- residual_in: bfloat16 [16384, 2048], P('sp'), may hold values from -6 to 6
- mixer_input: bfloat16 [2048, 16384], P('tp', 'sp'), may hold values from -6 to 6
- branch_gate: bfloat16 [2048, 16384], P('tp', 'sp'), may hold values from -6 to 6
- conv_taps: bfloat16 [2048, 4], P('tp'), may hold values from -3 to 3
- recur_weight: bfloat16 [32, 64, 64], P('tp'), may hold values from -0.75 to 0.75
- admit_weight: bfloat16 [32, 64, 64], P('tp'), may hold values from -0.75 to 0.75
- decay_param: float32 [2048], P('tp'), may hold values from 4 to 16
- decay_extra: float32 [2048, 16384], P('tp', 'sp'), may hold values from -1 to 0
- out_weight: bfloat16 [2048, 2048], P('tp'), may hold values from -0.375 to 0.375
- norm_gain: bfloat16 [2048], replicated, may hold values from 0.099609375 to 1.8984375
- gate_weight: bfloat16 [2048, 5632], P('sp', 'tp'), may hold values from -0.125 to 0.125
- up_weight: bfloat16 [2048, 5632], P('sp', 'tp'), may hold values from -0.125 to 0.125
- down_weight: bfloat16 [2048, 5632], P('sp', 'tp'), may hold values from -0.15625 to 0.15625
Outputs:
- layer_out: bfloat16 [16384, 2048], P('sp')
The draws below stay inside these ranges and needn't reach their ends.
All inputs are finite; a program needn't handle non-finite values.
Results may differ from the reference program's by a relative error of at most 0.019.
Values may be sent and summed in bfloat16 or wider, within the bound.
No kernel may reach another device: no remote copies, remote signals or barrier semaphores. Data moves between devices by JAX's collectives and lax.ppermute only.
A program may use at most 64 MiB of HBM per device.

```python
import jax
import jax.numpy as jnp
from jax import lax

D = 2048
W = 2048
BLOCKS = 32
BLOCK = 64
FF = 5632
KERNEL = 4
TOK_DEV = 256
TOKENS = 16384
N_SP = 64
N_TP = 8


def draw_decay_param(key, part):
    pick_key, slow_key, fast_key = jax.random.split(key, 3)
    slow_share = 0.5
    slow_rate = jax.random.uniform(slow_key, (W,), jnp.float32, 0.2, 0.6) / (4.0 * TOKENS)
    fast_rate = jnp.exp(jax.random.uniform(fast_key, (W,), jnp.float32, jnp.log(0.0025), jnp.log(0.01)))
    chosen = jax.random.uniform(pick_key, (W,), jnp.float32) < slow_share
    picked_rate = jnp.where(chosen, slow_rate, fast_rate)
    return (-jnp.log(jnp.expm1(picked_rate))).astype(jnp.float32)


def draw_decay_extra(key, part):
    level_key, spot_key, loss_key = jax.random.split(key, 3)
    low_end = 0.15
    high_end = 0.9
    block_count = TOKENS // TOK_DEV
    levels = jnp.exp(jax.random.uniform(level_key, (W, block_count), jnp.float32, jnp.log(low_end), jnp.log(high_end))) / TOKENS
    steady = -jnp.repeat(levels, TOK_DEV, axis=1)
    spots = jax.random.randint(spot_key, (3,), 0, TOKENS)
    losses = jnp.log1p(-jax.random.uniform(loss_key, (W, 3), jnp.float32, 0.2, 0.4))
    positions = jnp.arange(TOKENS)
    result_field = steady
    for which in range(3):
        hit_row = (positions == spots[which]).astype(jnp.float32)
        result_field = result_field + losses[:, which:which + 1] * hit_row[None, :]
    return result_field.astype(jnp.float32)


def shard_levels(key, shape, cuts, smallest, largest):
    loudness = 1.0
    for position, shards_of in cuts:
        steps = jax.random.uniform(jax.random.fold_in(jax.random.fold_in(key, 6), position), (shards_of,), jnp.float32, smallest / len(cuts), largest / len(cuts))
        loudness = loudness * jnp.repeat(jnp.exp(steps), shape[position] // shards_of).reshape((-1,) + (1,) * (len(shape) - 1 - position))
    return loudness


def normal_values(stream_key, shape, deviation, most, pieces=(), held_as=jnp.bfloat16):
    factor_of = shard_levels(stream_key, shape, pieces, -0.22, 0.18) if pieces else 1.0
    drawn = jax.random.normal(stream_key, shape, jnp.float32) * deviation * factor_of
    return jnp.minimum(jnp.maximum(drawn, -most), most).astype(held_as)


def setup_inputs(seed: int = 0) -> dict:
    keys = jax.random.split(jax.random.key(seed), 14)
    return {
        "residual_in": normal_values(keys[0], (TOKENS, D), 1.0, 6.0, ((0, 64),)),
        "mixer_input": normal_values(keys[1], (W, TOKENS), 1.0, 6.0, ((0, 8), (1, 64))),
        "branch_gate": normal_values(keys[2], (W, TOKENS), 1.0, 6.0, ((0, 8), (1, 64))),
        "conv_taps": normal_values(keys[3], (W, KERNEL), KERNEL ** -0.5, 3.0, ((0, 8),)),
        "recur_weight": normal_values(keys[4], (BLOCKS, BLOCK, BLOCK), BLOCK ** -0.5, 0.75, ((0, 8),)),
        "admit_weight": normal_values(keys[5], (BLOCKS, BLOCK, BLOCK), BLOCK ** -0.5, 0.75, ((0, 8),)),
        "decay_param": draw_decay_param(jax.random.fold_in(keys[13], 71), 0),
        "decay_extra": draw_decay_extra(jax.random.fold_in(keys[13], 71), 0),
        "out_weight": normal_values(keys[8], (W, D), (W // 8) ** -0.5, 0.375, ((0, 8),)),
        "norm_gain": jnp.clip(1.0 + 0.18 * jax.random.normal(keys[9], (D,), jnp.float32), 0.099609375, 1.8984375).astype(jnp.bfloat16),
        "gate_weight": normal_values(keys[10], (D, FF), D ** -0.5, 0.125, ((0, 64), (1, 8))),
        "up_weight": normal_values(keys[11], (D, FF), D ** -0.5, 0.125, ((0, 64), (1, 8))),
        "down_weight": normal_values(keys[12], (D, FF), (FF // 4) ** -0.5, 0.15625, ((0, 64), (1, 8))),
    }


def block_gates(weight, signal):
    groups = weight.shape[0]
    grouped = signal.astype(jnp.float32).reshape(groups, weight.shape[1], signal.shape[1])
    mapped = jnp.einsum('gij,git->gjt', weight.astype(jnp.float32), grouped)
    return jax.nn.sigmoid(mapped.reshape(signal.shape))

def link_pairs(earlier, latter):
    return (earlier[0] * latter[0], latter[0] * earlier[1] + latter[1])

def reference(residual_in, mixer_input, branch_gate, conv_taps, recur_weight, admit_weight, decay_param, decay_extra, out_weight, norm_gain, gate_weight, up_weight, down_weight):
    tap_count = conv_taps.shape[1]
    length = mixer_input.shape[1]
    padded = jnp.pad(mixer_input.astype(jnp.float32), ((0, 0), (tap_count - 1, 0)))
    tap_values = conv_taps.astype(jnp.float32)
    conv_sum = jnp.zeros(mixer_input.shape, jnp.float32)
    for tap in range(tap_count):
        conv_sum = conv_sum + tap_values[:, tap:tap + 1] * padded[:, tap:tap + length]
    conv_out = conv_sum.astype(jnp.bfloat16)
    recur_gate = block_gates(recur_weight, conv_out)
    admit_gate = block_gates(admit_weight, conv_out)
    base_rate = jax.nn.softplus(-decay_param.astype(jnp.float32))[:, None]
    log_decay = -8.0 * recur_gate * base_rate + decay_extra
    decay_step = jnp.exp(log_decay)
    drive_term = jnp.sqrt(-jnp.expm1(2.0 * log_decay)) * admit_gate * conv_out.astype(jnp.float32)
    running, states = lax.associative_scan(link_pairs, (decay_step, drive_term), axis=1)
    gate_act = jax.nn.gelu(branch_gate.astype(jnp.float32), approximate=True)
    mixed_out = (states * gate_act).astype(jnp.bfloat16)
    model_width = residual_in.shape[1]
    split_width = gate_weight.shape[1] // N_TP
    res_blocks = residual_in.reshape(N_SP, TOK_DEV, model_width)
    mix_blocks = mixed_out.reshape(mixed_out.shape[0], N_SP, TOK_DEV).transpose(1, 0, 2)
    gain_wide = norm_gain.astype(jnp.float32)
    down_split = down_weight.astype(jnp.float32).reshape(model_width, N_TP, split_width)

    def one_block(pair):
        resid, mix_block = pair
        branch = jnp.dot(mix_block.T, out_weight, preferred_element_type=jnp.float32)
        middle = (resid.astype(jnp.float32) + branch).astype(jnp.bfloat16)
        middle_wide = middle.astype(jnp.float32)
        row_scale = lax.rsqrt(lax.optimization_barrier(jnp.mean(middle_wide * middle_wide, axis=1, keepdims=True)) + 1e-06)
        normed = (middle_wide * row_scale * gain_wide).astype(jnp.bfloat16)
        gate_pre = jnp.dot(normed, gate_weight, preferred_element_type=jnp.float32)
        up_pre = jnp.dot(normed, up_weight, preferred_element_type=jnp.float32)
        hidden = (jax.nn.silu(gate_pre) * up_pre).astype(jnp.bfloat16)
        hidden_split = hidden.astype(jnp.float32).reshape(hidden.shape[0], N_TP, split_width)
        partial_value = jnp.einsum('tkf,dkf->ktd', hidden_split, down_split).astype(jnp.bfloat16)
        partial_value = lax.optimization_barrier(partial_value)
        channel_out = lax.optimization_barrier(jnp.sum(partial_value.astype(jnp.float32), axis=0))
        return (middle.astype(jnp.float32) + channel_out).astype(jnp.bfloat16)
    layer_blocks = lax.map(one_block, (res_blocks, mix_blocks))
    return layer_blocks.reshape(N_SP * TOK_DEV, model_width)
```

```python
import jax
import jax.numpy as jnp
from jax import lax
from jax.experimental import pallas as pl
from jax.experimental.pallas import tpu as pltpu
from jax.sharding import Mesh
from jax.sharding import PartitionSpec as P

SP = ("z", "y")
TP = ("x", "core")


def shifted(value, by, fill):
    rows = value.shape[0]
    head = jnp.full((by, value.shape[1]), fill, value.dtype)
    if by % 8 == 0:
        return jnp.concatenate([head, value[: rows - by]], axis=0)
    rolled = pltpu.roll(value, by, 0)
    row = lax.broadcasted_iota(jnp.int32, value.shape, 0)
    return jnp.where(row < by, jnp.asarray(fill, value.dtype), rolled)


def recurrence_body(
    mixer, before, taps, recur, admit, rate, extra, branch, scale_out, shift_out, ends_out
):
    channels, length = mixer.shape
    tap_count = taps.shape[1]
    signal = mixer[...].astype(jnp.float32).T
    eye = (
        lax.broadcasted_iota(jnp.int32, (channels, channels), 0)
        == lax.broadcasted_iota(jnp.int32, (channels, channels), 1)
    ).astype(jnp.bfloat16)
    turn = (((0,), (0,)), ((), ()))
    tap_rows = lax.dot_general(taps[...], eye, turn, preferred_element_type=jnp.float32)
    halo = lax.dot_general(before[...], eye, turn, preferred_element_type=jnp.float32)
    row = lax.broadcasted_iota(jnp.int32, signal.shape, 0)
    conv_sum = jnp.zeros(signal.shape, jnp.float32)
    for tap in range(tap_count):
        back = tap_count - 1 - tap
        moved = signal
        if back:
            moved = pltpu.roll(signal, back, 0)
            for line in range(back):
                moved = jnp.where(row == line, halo[tap + line : tap + line + 1], moved)
        conv_sum = conv_sum + tap_rows[tap : tap + 1] * moved
    conv_out = conv_sum.astype(jnp.bfloat16)
    groups, width, _ = recur.shape
    spread = (
        lax.broadcasted_iota(jnp.int32, (width, channels), 1) % width
        == lax.broadcasted_iota(jnp.int32, (width, channels), 0)
    ).astype(jnp.bfloat16)
    same = (
        lax.broadcasted_iota(jnp.int32, (channels, channels), 0) // width
        == lax.broadcasted_iota(jnp.int32, (channels, channels), 1) // width
    )

    def gate(weight):
        flat = weight[...].reshape(groups * width, width)
        wide = jnp.dot(flat, spread, preferred_element_type=jnp.float32)
        wide = jnp.where(same, wide, 0.0).astype(jnp.bfloat16)
        return jax.nn.sigmoid(jnp.dot(conv_out, wide, preferred_element_type=jnp.float32))

    recur_gate = gate(recur)
    admit_gate = gate(admit)
    log_decay = -8.0 * recur_gate * rate[...] + extra[...].T
    run = jnp.exp(log_decay)
    twice = 2.0 * log_decay
    series = twice * (1.0 + twice * (0.5 + twice * (1.0 / 6.0 + twice * (1.0 / 24.0 + twice * (
        1.0 / 120.0 + twice * (1.0 / 720.0))))))
    lost = -jnp.where(twice > -0.25, series, run * run - 1.0)
    kept = jnp.where(lost > 0.0, jnp.sqrt(lost), 0.0)
    state = kept * admit_gate * conv_out.astype(jnp.float32)
    by = 1
    while by < length:
        state = state + run * shifted(state, by, 0.0)
        run = run * shifted(run, by, 1.0)
        by *= 2
    ends_out[0:1] = run[length - 1 : length]
    ends_out[1:2] = state[length - 1 : length]
    gelu = jax.nn.gelu(branch[...].astype(jnp.float32), approximate=True).T
    scale_out[...] = run * gelu
    shift_out[...] = state * gelu


def carry_body(place, ends, scale, shift, weight, send, keep):
    count = ends.shape[0]
    mine, core = place[0], place[1]
    half = send.shape[0]
    entering = jnp.zeros((1, scale.shape[1]), jnp.float32)
    for k in range(count):
        pair = ends[k]
        after = pair[0:1] * entering + pair[1:2]
        entering = jnp.where(k < mine, after, entering)
    for target, side in ((send, 1 - core), (keep, core)):
        at = pl.ds(pl.multiple_of(side * half, half), half)
        mixed = (shift[at, :] + scale[at, :] * entering).astype(jnp.bfloat16)
        found = jnp.dot(mixed, weight[...], preferred_element_type=jnp.float32)
        target[...] = found.astype(jnp.bfloat16)


def norm_body(place, residual, arrived, gain, own, normed):
    share = own.shape[0]
    branch = arrived[0].astype(jnp.float32)
    for k in range(1, arrived.shape[0]):
        branch = branch + arrived[k].astype(jnp.float32)
    at = pl.ds(pl.multiple_of(place[0], share), share)
    middle = (residual[at, :].astype(jnp.float32) + branch).astype(jnp.bfloat16)
    own[...] = middle
    wide = middle.astype(jnp.float32)
    row_scale = lax.rsqrt(jnp.mean(wide * wide, axis=1, keepdims=True) + 1e-06)
    normed[...] = (wide * row_scale * gain[...].astype(jnp.float32)).astype(jnp.bfloat16)


def feed_body(near, far, weights, send, keep, both_sum, down, hidden):
    step = pl.program_id(0)
    parts = down.shape[0]
    half = near.shape[0]
    units = hidden.shape[1]
    span = weights.shape[0]
    both = weights[:, : 2 * units]
    down[step] = weights[:, 2 * units :]

    @pl.when(step == 0)
    def _():
        for at, piece in ((0, near), (half, far)):
            found = jnp.dot(piece[...], both, preferred_element_type=jnp.float32)
            both_sum[pl.ds(at, half), :] = found

    @pl.when(step > 0)
    def _():
        for at, piece in ((0, near), (half, far)):
            found = jnp.dot(piece[...], both, preferred_element_type=jnp.float32)
            both_sum[pl.ds(at, half), :] += found

    @pl.when(step == parts - 1)
    def _():
        gated = both_sum[:, :units]
        silu = gated / (1.0 + jnp.exp(-gated))
        hidden[...] = (silu * both_sum[:, units:]).astype(jnp.bfloat16)
        flip = (((1,), (1,)), ((), ()))
        for k in range(parts):
            found = lax.dot_general(hidden[...], down[k], flip, preferred_element_type=jnp.float32)
            keep[:, k * span : (k + 1) * span] = found[:half].astype(jnp.bfloat16)
            send[:, k * span : (k + 1) * span] = found[half:].astype(jnp.bfloat16)


def whole(shape):
    return pl.BlockSpec(shape, lambda *_: (0,) * len(shape))


def swap_cores(value):
    return lax.ppermute(value, "core", [(0, 1), (1, 0)])


def on_device(
    residual_in,
    mixer_input,
    branch_gate,
    conv_taps,
    recur_weight,
    admit_weight,
    decay_param,
    decay_extra,
    out_weight,
    norm_gain,
    gate_weight,
    up_weight,
    down_weight,
):
    units = gate_weight.shape[1]
    weights = jnp.concatenate([gate_weight, up_weight, down_weight], axis=1)
    weights = lax.all_gather(weights, SP, axis=0, tiled=True)

    channels, length = mixer_input.shape
    tap_count = conv_taps.shape[1]
    count = lax.axis_size(SP)
    tail = mixer_input[:, length - (tap_count - 1) :]
    before = lax.ppermute(tail, SP, [(i, i + 1) for i in range(count - 1)])
    square = jax.ShapeDtypeStruct((length, channels), jnp.float32)
    scale, shift, ends = pl.pallas_call(
        recurrence_body,
        out_shape=(square, square, jax.ShapeDtypeStruct((2, channels), jnp.float32)),
        in_specs=[pl.BlockSpec(memory_space=pltpu.VMEM)] * 8,
        out_specs=(pl.BlockSpec(memory_space=pltpu.VMEM),) * 3,
        name="recurrence",
    )(
        mixer_input,
        before,
        conv_taps,
        recur_weight,
        admit_weight,
        jax.nn.softplus(-decay_param).reshape(1, channels),
        decay_extra,
        branch_gate,
    )
    everyone = lax.all_to_all(
        jnp.broadcast_to(ends[None], (count, *ends.shape)), SP, 0, 0, tiled=True
    )
    core = lax.axis_index("core")
    place = jnp.stack([lax.axis_index(SP), core]).astype(jnp.int32)
    half = length // 2
    width = out_weight.shape[1]
    ring = lax.axis_size("x")
    share = half // ring
    half_shape = jax.ShapeDtypeStruct((half, width), jnp.bfloat16)
    share_shape = jax.ShapeDtypeStruct((share, width), jnp.bfloat16)
    smem = pl.BlockSpec(memory_space=pltpu.SMEM)
    vmem = pl.BlockSpec(memory_space=pltpu.VMEM)
    send, keep = pl.pallas_call(
        carry_body,
        out_shape=(half_shape, half_shape),
        in_specs=[smem] + [vmem] * 4,
        out_specs=(vmem, vmem),
        name="carry",
    )(place, everyone, scale, shift, out_weight)

    def to_owners(keep, send):
        paired = keep.astype(jnp.float32) + swap_cores(send).astype(jnp.float32)
        tiles = paired.astype(jnp.bfloat16).reshape(ring, share, width)
        return lax.all_to_all(tiles, "x", split_axis=0, concat_axis=0, tiled=True)

    spot = (core * half + lax.axis_index("x") * share).astype(jnp.int32).reshape(1)
    own, normed = pl.pallas_call(
        norm_body,
        out_shape=(share_shape, share_shape),
        in_specs=[smem] + [vmem] * 3,
        out_specs=(vmem, vmem),
        name="norm",
    )(spot, residual_in, to_owners(keep, send), norm_gain.reshape(1, width))
    near = lax.all_gather(normed, "x", axis=0, tiled=True)
    far = swap_cores(near)

    parts = 4
    span = width // parts
    rows_block = pl.BlockSpec((half, span), lambda i: (0, i))
    send, keep = pl.pallas_call(
        feed_body,
        grid=(parts,),
        out_shape=(half_shape, half_shape),
        in_specs=[
            rows_block,
            rows_block,
            pl.BlockSpec((span, 3 * units), lambda i: (i, 0)),
        ],
        out_specs=(whole((half, width)), whole((half, width))),
        scratch_shapes=[
            pltpu.VMEM((length, 2 * units), jnp.float32),
            pltpu.VMEM((parts, span, units), jnp.bfloat16),
            pltpu.VMEM((length, units), jnp.bfloat16),
        ],
        name="feed",
    )(near, far, weights)
    channel_out = to_owners(keep, send).astype(jnp.float32).sum(axis=0)
    layer_rows = (own.astype(jnp.float32) + channel_out).astype(jnp.bfloat16)
    side = lax.all_gather(layer_rows, "x", axis=0, tiled=True)
    other = swap_cores(side)
    low = jnp.where(core == 0, side, other)
    high = jnp.where(core == 0, other, side)
    return jnp.concatenate([low, high], axis=0)


def solution(mesh):
    sizes = (8, mesh.shape["sp"] // 8, mesh.shape["tp"] // 2, 2)
    torus = Mesh(mesh.devices.reshape(sizes), ("z", "y", "x", "core"))
    in_specs = (
        P(SP, None),
        P(TP, SP),
        P(TP, SP),
        P(TP, None),
        P(TP, None, None),
        P(TP, None, None),
        P(TP),
        P(TP, SP),
        P(TP, None),
        P(),
        P(SP, TP),
        P(SP, TP),
        P(SP, TP),
    )
    return jax.shard_map(
        on_device, mesh=torus, in_specs=in_specs, out_specs=P(SP, None), check_vma=False
    )
```

```python
import jax
import jax.numpy as jnp
from jax import lax
from jax.experimental import pallas as pl
from jax.experimental.pallas import tpu as pltpu
from jax.sharding import Mesh
from jax.sharding import PartitionSpec as P

SP = ("z", "y")
TP = ("x", "core")


def shifted(value, by, fill):
    rows = value.shape[0]
    head = jnp.full((by, value.shape[1]), fill, value.dtype)
    if by % 8 == 0:
        return jnp.concatenate([head, value[: rows - by]], axis=0)
    rolled = pltpu.roll(value, by, 0)
    row = lax.broadcasted_iota(jnp.int32, value.shape, 0)
    return jnp.where(row < by, jnp.asarray(fill, value.dtype), rolled)


def recurrence_body(
    mixer, before, taps, recur, admit, rate, extra, branch, scale_out, shift_out, ends_out
):
    channels, length = mixer.shape
    tap_count = taps.shape[1]
    signal = mixer[...].astype(jnp.float32).T
    eye = (
        lax.broadcasted_iota(jnp.int32, (channels, channels), 0)
        == lax.broadcasted_iota(jnp.int32, (channels, channels), 1)
    ).astype(jnp.bfloat16)
    turn = (((0,), (0,)), ((), ()))
    tap_rows = lax.dot_general(taps[...], eye, turn, preferred_element_type=jnp.float32)
    halo = lax.dot_general(before[...], eye, turn, preferred_element_type=jnp.float32)
    row = lax.broadcasted_iota(jnp.int32, signal.shape, 0)
    conv_sum = jnp.zeros(signal.shape, jnp.float32)
    for tap in range(tap_count):
        back = tap_count - 1 - tap
        moved = signal
        if back:
            moved = pltpu.roll(signal, back, 0)
            for line in range(back):
                moved = jnp.where(row == line, halo[tap + line : tap + line + 1], moved)
        conv_sum = conv_sum + tap_rows[tap : tap + 1] * moved
    conv_out = conv_sum.astype(jnp.bfloat16)
    groups, width, _ = recur.shape
    spread = (
        lax.broadcasted_iota(jnp.int32, (width, channels), 1) % width
        == lax.broadcasted_iota(jnp.int32, (width, channels), 0)
    ).astype(jnp.bfloat16)
    same = (
        lax.broadcasted_iota(jnp.int32, (channels, channels), 0) // width
        == lax.broadcasted_iota(jnp.int32, (channels, channels), 1) // width
    )

    def gate(weight):
        flat = weight[...].reshape(groups * width, width)
        wide = jnp.dot(flat, spread, preferred_element_type=jnp.float32)
        wide = jnp.where(same, wide, 0.0).astype(jnp.bfloat16)
        return jax.nn.sigmoid(jnp.dot(conv_out, wide, preferred_element_type=jnp.float32))

    recur_gate = gate(recur)
    admit_gate = gate(admit)
    log_decay = -8.0 * recur_gate * rate[...] + extra[...].T
    run = jnp.exp(log_decay)
    twice = 2.0 * log_decay
    series = twice * (1.0 + twice * (0.5 + twice * (1.0 / 6.0 + twice * (1.0 / 24.0 + twice * (
        1.0 / 120.0 + twice * (1.0 / 720.0))))))
    lost = -jnp.where(twice > -0.25, series, run * run - 1.0)
    kept = jnp.where(lost > 0.0, jnp.sqrt(lost), 0.0)
    state = kept * admit_gate * conv_out.astype(jnp.float32)
    by = 1
    while by < length:
        state = state + run * shifted(state, by, 0.0)
        run = run * shifted(run, by, 1.0)
        by *= 2
    ends_out[0:1] = run[length - 1 : length]
    ends_out[1:2] = state[length - 1 : length]
    gelu = jax.nn.gelu(branch[...].astype(jnp.float32), approximate=True).T
    scale_out[...] = run * gelu
    shift_out[...] = state * gelu


def carry_body(place, ends, scale, shift, weight, send, keep):
    count = ends.shape[0]
    mine, core = place[0], place[1]
    half = send.shape[0]
    entering = jnp.zeros((1, scale.shape[1]), jnp.float32)
    for k in range(count):
        pair = ends[k]
        after = pair[0:1] * entering + pair[1:2]
        entering = jnp.where(k < mine, after, entering)
    for target, side in ((send, 1 - core), (keep, core)):
        at = pl.ds(pl.multiple_of(side * half, half), half)
        mixed = (shift[at, :] + scale[at, :] * entering).astype(jnp.bfloat16)
        found = jnp.dot(mixed, weight[...], preferred_element_type=jnp.float32)
        target[...] = found.astype(jnp.bfloat16)


def norm_body(place, residual, low, low_came, high, high_came, gain, middle, normed):
    half = middle.shape[0]
    quarter = half // 2
    for at, mine, came in ((0, low, low_came), (quarter, high, high_came)):
        branch = mine[...].astype(jnp.float32) + came[...].astype(jnp.float32)
        rows = pl.ds(pl.multiple_of(place[1] * half + at, quarter), quarter)
        found = (residual[rows, :].astype(jnp.float32) + branch).astype(jnp.bfloat16)
        middle[at : at + quarter, :] = found
        wide = found.astype(jnp.float32)
        row_scale = lax.rsqrt(jnp.mean(wide * wide, axis=1, keepdims=True) + 1e-06)
        ready = wide * row_scale * gain[...].astype(jnp.float32)
        normed[at : at + quarter, :] = ready.astype(jnp.bfloat16)


def feed_body(near, far, weights, send, keep, rows, stage, both_sum, hidden, arrived):
    parts, span, _ = stage.shape
    half = near.shape[0]
    units = hidden.shape[1]
    copies = [
        pltpu.make_async_copy(weights.at[pl.ds(k * span, span), :], stage.at[k], arrived.at[k])
        for k in range(parts)
    ]
    for copy in copies:
        copy.start()
    rows[:half] = near[...]
    rows[half:] = far[...]
    for k in range(parts):
        copies[k].wait()
        piece = rows[:, k * span : (k + 1) * span]
        found = jnp.dot(piece, stage[k, :, : 2 * units], preferred_element_type=jnp.float32)
        if k == 0:
            both_sum[...] = found
        else:
            both_sum[...] += found
    gated = both_sum[:, :units]
    silu = gated / (1.0 + jnp.exp(-gated))
    hidden[...] = (silu * both_sum[:, units:]).astype(jnp.bfloat16)
    flip = (((1,), (1,)), ((), ()))
    for k in range(parts):
        down = stage[k, :, 2 * units :]
        found = lax.dot_general(hidden[...], down, flip, preferred_element_type=jnp.float32)
        keep[:, k * span : (k + 1) * span] = found[:half].astype(jnp.bfloat16)
        send[:, k * span : (k + 1) * span] = found[half:].astype(jnp.bfloat16)


def swap_cores(value):
    return lax.ppermute(value, "core", [(0, 1), (1, 0)])


def on_device(
    residual_in,
    mixer_input,
    branch_gate,
    conv_taps,
    recur_weight,
    admit_weight,
    decay_param,
    decay_extra,
    out_weight,
    norm_gain,
    gate_weight,
    up_weight,
    down_weight,
):
    units = gate_weight.shape[1]
    weights = jnp.concatenate([gate_weight, up_weight, down_weight], axis=1)
    weights = lax.all_gather(weights, SP, axis=0, tiled=True)

    channels, length = mixer_input.shape
    tap_count = conv_taps.shape[1]
    count = lax.axis_size(SP)
    tail = mixer_input[:, length - (tap_count - 1) :]
    before = lax.ppermute(tail, SP, [(i, i + 1) for i in range(count - 1)])
    square = jax.ShapeDtypeStruct((length, channels), jnp.float32)
    scale, shift, ends = pl.pallas_call(
        recurrence_body,
        out_shape=(square, square, jax.ShapeDtypeStruct((2, channels), jnp.float32)),
        in_specs=[pl.BlockSpec(memory_space=pltpu.VMEM)] * 8,
        out_specs=(pl.BlockSpec(memory_space=pltpu.VMEM),) * 3,
        name="recurrence",
    )(
        mixer_input,
        before,
        conv_taps,
        recur_weight,
        admit_weight,
        jax.nn.softplus(-decay_param).reshape(1, channels),
        decay_extra,
        branch_gate,
    )
    everyone = lax.all_to_all(
        jnp.broadcast_to(ends[None], (count, *ends.shape)), SP, 0, 0, tiled=True
    )
    core = lax.axis_index("core")
    place = jnp.stack([lax.axis_index(SP), core]).astype(jnp.int32)
    half = length // 2
    width = out_weight.shape[1]
    half_shape = jax.ShapeDtypeStruct((half, width), jnp.bfloat16)
    smem = pl.BlockSpec(memory_space=pltpu.SMEM)
    vmem = pl.BlockSpec(memory_space=pltpu.VMEM)
    send, keep = pl.pallas_call(
        carry_body,
        out_shape=(half_shape, half_shape),
        in_specs=[smem] + [vmem] * 4,
        out_specs=(vmem, vmem),
        name="carry",
    )(place, everyone, scale, shift, out_weight)

    quarter = half // 2
    even = [(0, 1), (1, 0), (2, 3), (3, 2)]
    odd = [(1, 2), (2, 1), (3, 0), (0, 3)]

    def added(mine, came):
        return (mine.astype(jnp.float32) + came.astype(jnp.float32)).astype(jnp.bfloat16)

    def summed(keep, send):
        came = swap_cores(send)
        low = added(keep[:quarter], came[:quarter])
        high = added(keep[quarter:], came[quarter:])
        low_came = lax.ppermute(low, "x", even)
        high_came = lax.ppermute(high, "x", odd)
        low = added(low, low_came)
        high = added(high, high_came)
        return low, lax.ppermute(low, "x", odd), high, lax.ppermute(high, "x", even)

    middle, near = pl.pallas_call(
        norm_body,
        out_shape=(half_shape, half_shape),
        in_specs=[smem] + [vmem] * 6,
        out_specs=(vmem, vmem),
        name="norm",
    )(place, residual_in, *summed(keep, send), norm_gain.reshape(1, width))
    far = swap_cores(near)

    parts = 4
    span = width // parts
    send, keep = pl.pallas_call(
        feed_body,
        out_shape=(half_shape, half_shape),
        in_specs=[vmem, vmem, pl.BlockSpec(memory_space=pl.ANY)],
        out_specs=(vmem, vmem),
        scratch_shapes=[
            pltpu.VMEM((length, width), jnp.bfloat16),
            pltpu.VMEM((parts, span, 3 * units), jnp.bfloat16),
            pltpu.VMEM((length, 2 * units), jnp.float32),
            pltpu.VMEM((length, units), jnp.bfloat16),
            pltpu.SemaphoreType.DMA((parts,)),
        ],
        name="feed",
    )(near, far, weights)
    low, low_came, high, high_came = summed(keep, send)

    def finished(rows, mine, came):
        channel_out = mine.astype(jnp.float32) + came.astype(jnp.float32)
        own = (rows.astype(jnp.float32) + channel_out).astype(jnp.bfloat16)
        return own, swap_cores(own)

    low, low_other = finished(middle[:quarter], low, low_came)
    high, high_other = finished(middle[quarter:], high, high_came)
    mine = (low, high)
    other = (low_other, high_other)
    first = [jnp.where(core == 0, a, b) for a, b in zip(mine, other)]
    last = [jnp.where(core == 0, b, a) for a, b in zip(mine, other)]
    return jnp.concatenate(first + last, axis=0)


def solution(mesh):
    sizes = (8, mesh.shape["sp"] // 8, mesh.shape["tp"] // 2, 2)
    torus = Mesh(mesh.devices.reshape(sizes), ("z", "y", "x", "core"))
    in_specs = (
        P(SP, None),
        P(TP, SP),
        P(TP, SP),
        P(TP, None),
        P(TP, None, None),
        P(TP, None, None),
        P(TP),
        P(TP, SP),
        P(TP, None),
        P(),
        P(SP, TP),
        P(SP, TP),
        P(SP, TP),
    )
    return jax.shard_map(
        on_device, mesh=torus, in_specs=in_specs, out_specs=P(SP, None), check_vma=False
    )
```

```python
import functools

import jax
import jax.numpy as jnp
from jax import lax
from jax.experimental import pallas as pl
from jax.experimental.pallas import tpu as pltpu
from jax.sharding import Mesh
from jax.sharding import PartitionSpec as P

SP = ("z", "y")
TP = ("x", "core")


def shifted(value, by, fill):
    rows = value.shape[0]
    head = jnp.full((by, value.shape[1]), fill, value.dtype)
    if by % 8 == 0:
        return jnp.concatenate([head, value[: rows - by]], axis=0)
    rolled = pltpu.roll(value, by, 0)
    row = lax.broadcasted_iota(jnp.int32, value.shape, 0)
    return jnp.where(row < by, jnp.asarray(fill, value.dtype), rolled)


def recurrence_body(
    mixer, before, taps, recur, admit, rate, extra, branch, scale_out, shift_out, ends_out
):
    channels, length = mixer.shape
    tap_count = taps.shape[1]
    signal = mixer[...].astype(jnp.float32).T
    eye = (
        lax.broadcasted_iota(jnp.int32, (channels, channels), 0)
        == lax.broadcasted_iota(jnp.int32, (channels, channels), 1)
    ).astype(jnp.bfloat16)
    turn = (((0,), (0,)), ((), ()))
    tap_rows = lax.dot_general(taps[...], eye, turn, preferred_element_type=jnp.float32)
    halo = lax.dot_general(before[...], eye, turn, preferred_element_type=jnp.float32)
    row = lax.broadcasted_iota(jnp.int32, signal.shape, 0)
    conv_sum = jnp.zeros(signal.shape, jnp.float32)
    for tap in range(tap_count):
        back = tap_count - 1 - tap
        moved = signal
        if back:
            moved = pltpu.roll(signal, back, 0)
            for line in range(back):
                moved = jnp.where(row == line, halo[tap + line : tap + line + 1], moved)
        conv_sum = conv_sum + tap_rows[tap : tap + 1] * moved
    conv_out = conv_sum.astype(jnp.bfloat16)
    groups, width, _ = recur.shape
    spread = (
        lax.broadcasted_iota(jnp.int32, (width, channels), 1) % width
        == lax.broadcasted_iota(jnp.int32, (width, channels), 0)
    ).astype(jnp.bfloat16)
    same = (
        lax.broadcasted_iota(jnp.int32, (channels, channels), 0) // width
        == lax.broadcasted_iota(jnp.int32, (channels, channels), 1) // width
    )

    def gate(weight):
        flat = weight[...].reshape(groups * width, width)
        wide = jnp.dot(flat, spread, preferred_element_type=jnp.float32)
        wide = jnp.where(same, wide, 0.0).astype(jnp.bfloat16)
        return jax.nn.sigmoid(jnp.dot(conv_out, wide, preferred_element_type=jnp.float32))

    recur_gate = gate(recur)
    admit_gate = gate(admit)
    log_decay = -8.0 * recur_gate * rate[...] + extra[...].T
    run = jnp.exp(log_decay)
    twice = 2.0 * log_decay
    series = twice * (1.0 + twice * (0.5 + twice * (1.0 / 6.0 + twice * (1.0 / 24.0 + twice * (
        1.0 / 120.0 + twice * (1.0 / 720.0))))))
    lost = -jnp.where(twice > -0.25, series, run * run - 1.0)
    kept = jnp.where(lost > 0.0, jnp.sqrt(lost), 0.0)
    state = kept * admit_gate * conv_out.astype(jnp.float32)
    by = 1
    while by < length:
        state = state + run * shifted(state, by, 0.0)
        run = run * shifted(run, by, 1.0)
        by *= 2
    ends_out[0:1] = run[length - 1 : length]
    ends_out[1:2] = state[length - 1 : length]
    gelu = jax.nn.gelu(branch[...].astype(jnp.float32), approximate=True).T
    scale_out[...] = run * gelu
    shift_out[...] = state * gelu


def carry_body(place, ends, scale, shift, weight, send, keep):
    count = ends.shape[0]
    mine, core = place[0], place[1]
    half = send.shape[0]
    entering = jnp.zeros((1, scale.shape[1]), jnp.float32)
    for k in range(count):
        pair = ends[k]
        after = pair[0:1] * entering + pair[1:2]
        entering = jnp.where(k < mine, after, entering)
    for target, side in ((send, 1 - core), (keep, core)):
        at = pl.ds(pl.multiple_of(side * half, half), half)
        mixed = (shift[at, :] + scale[at, :] * entering).astype(jnp.bfloat16)
        found = jnp.dot(mixed, weight[...], preferred_element_type=jnp.float32)
        target[...] = found.astype(jnp.bfloat16)


def norm_body(place, residual, low, low_came, high, high_came, gain, middle, normed):
    half = middle.shape[0]
    quarter = half // 2
    for at, mine, came in ((0, low, low_came), (quarter, high, high_came)):
        branch = mine[...].astype(jnp.float32) + came[...].astype(jnp.float32)
        rows = pl.ds(pl.multiple_of(place[1] * half + at, quarter), quarter)
        found = (residual[rows, :].astype(jnp.float32) + branch).astype(jnp.bfloat16)
        middle[at : at + quarter, :] = found
        wide = found.astype(jnp.float32)
        row_scale = lax.rsqrt(jnp.mean(wide * wide, axis=1, keepdims=True) + 1e-06)
        ready = wide * row_scale * gain[...].astype(jnp.float32)
        normed[at : at + quarter, :] = ready.astype(jnp.bfloat16)


def feed_body(plan, place, near, far, *refs):
    left_from, right_from = plan
    left = refs[: len(left_from)]
    right = refs[len(left_from) : len(left_from) + len(right_from)]
    send, keep, rows, stage, left_sum, hidden = refs[len(left_from) + len(right_from) :]
    turns, length, span = rows.shape
    half = near.shape[0]
    units = hidden.shape[1]
    over = 2 * units - left_sum.shape[1]
    z, y = place[2], place[3]
    for k in range(turns):
        rows[k, :half] = near[:, k * span : (k + 1) * span]
        rows[k, half:] = far[:, k * span : (k + 1) * span]
    for ref, by in zip(right, right_from):
        line = lax.rem(y + (by + stage.shape[1]), stage.shape[1])
        for k in range(turns):
            stage[k, line] = ref[k]
    for k in range(0, len(left), 2):
        found = None
        for ref, by in zip(left[k : k + 2], left_from[k : k + 2]):
            piece = rows[lax.rem(z + (by + turns), turns)]
            weight = ref[...].reshape(span, ref.shape[2])
            part = jnp.dot(piece, weight, preferred_element_type=jnp.float32)
            found = part if found is None else found + part
        if k == 0:
            left_sum[...] = found
        else:
            left_sum[...] += found
    right_sum = None
    for k in range(turns):
        weight = stage[k, :, :, :over].reshape(span, over)
        part = jnp.dot(rows[k], weight, preferred_element_type=jnp.float32)
        right_sum = part if right_sum is None else right_sum + part
    gated = left_sum[:, :units]
    silu = gated / (1.0 + jnp.exp(-gated))
    up = jnp.concatenate([left_sum[:, units:], right_sum], axis=1)
    hidden[...] = (silu * up).astype(jnp.bfloat16)
    flip = (((1,), (1,)), ((), ()))
    for k in range(turns):
        down = stage[k, :, :, over:].reshape(span, units)
        found = lax.dot_general(hidden[...], down, flip, preferred_element_type=jnp.float32)
        keep[:, k * span : (k + 1) * span] = found[:half].astype(jnp.bfloat16)
        send[:, k * span : (k + 1) * span] = found[half:].astype(jnp.bfloat16)


def stack_body(offsets, place, *refs):
    out = refs[-1]
    for ref, by in zip(refs[:-1], offsets):
        out[lax.rem(place[0] + (by + out.shape[0]), out.shape[0])] = ref[...]


def sent_to_all(value, axis):
    count = lax.axis_size(axis)
    return lax.all_to_all(
        jnp.broadcast_to(value[None], (count, *value.shape)), axis, 0, 0, tiled=True
    )


def both_ways(block, axis, ahead, behind):
    count = lax.axis_size(axis)
    found, ups, downs = [(block, 0)], block, block
    for k in range(1, max(ahead, behind) + 1):
        if k <= ahead:
            ups = lax.ppermute(ups, axis, [(i, (i + 1) % count) for i in range(count)])
            found.append((ups, -k))
        if k <= behind:
            downs = lax.ppermute(downs, axis, [(i, (i - 1) % count) for i in range(count)])
            found.append((downs, k))
    return found


def swap_cores(value):
    return lax.ppermute(value, "core", [(0, 1), (1, 0)])


def on_device(
    residual_in,
    mixer_input,
    branch_gate,
    conv_taps,
    recur_weight,
    admit_weight,
    decay_param,
    decay_extra,
    out_weight,
    norm_gain,
    gate_weight,
    up_weight,
    down_weight,
):
    units = gate_weight.shape[1]
    cut = 448
    left = jnp.concatenate([gate_weight, up_weight[:, :cut]], axis=1)
    right = jnp.concatenate([up_weight[:, cut:], down_weight], axis=1)
    column = sent_to_all(right, "z")
    around = both_ways(left, "y", 4, 3)
    y_place = lax.axis_index("y").astype(jnp.int32).reshape(1)
    smem = pl.BlockSpec(memory_space=pltpu.SMEM)
    vmem = pl.BlockSpec(memory_space=pltpu.VMEM)
    row = pl.pallas_call(
        functools.partial(stack_body, tuple(by for _, by in around)),
        out_shape=jax.ShapeDtypeStruct((len(around), *left.shape), left.dtype),
        in_specs=[smem] + [vmem] * len(around),
        out_specs=vmem,
        compiler_params=pltpu.CompilerParams(vmem_limit_bytes=8 * 1024 * 1024),
        name="stack",
    )(y_place, *(pltpu.with_memory_space_constraint(b, pltpu.VMEM) for b, _ in around))
    left = both_ways(row, "z", 4, 3)
    right = both_ways(column, "y", 3, 4)

    channels, length = mixer_input.shape
    tap_count = conv_taps.shape[1]
    count = lax.axis_size(SP)
    tail = mixer_input[:, length - (tap_count - 1) :]
    before = lax.ppermute(tail, SP, [(i, i + 1) for i in range(count - 1)])
    square = jax.ShapeDtypeStruct((length, channels), jnp.float32)
    scale, shift, ends = pl.pallas_call(
        recurrence_body,
        out_shape=(square, square, jax.ShapeDtypeStruct((2, channels), jnp.float32)),
        in_specs=[pl.BlockSpec(memory_space=pltpu.VMEM)] * 8,
        out_specs=(pl.BlockSpec(memory_space=pltpu.VMEM),) * 3,
        compiler_params=pltpu.CompilerParams(vmem_limit_bytes=16 * 1024 * 1024),
        name="recurrence",
    )(
        mixer_input,
        before,
        conv_taps,
        recur_weight,
        admit_weight,
        jax.nn.softplus(-decay_param).reshape(1, channels),
        decay_extra,
        branch_gate,
    )
    ends, _ = lax.optimization_barrier((ends, column))
    everyone = sent_to_all(ends, SP)
    core = lax.axis_index("core")
    place = jnp.stack([lax.axis_index(SP), core, lax.axis_index("z"), lax.axis_index("y")])
    half = length // 2
    width = out_weight.shape[1]
    half_shape = jax.ShapeDtypeStruct((half, width), jnp.bfloat16)
    send, keep = pl.pallas_call(
        carry_body,
        out_shape=(half_shape, half_shape),
        in_specs=[smem] + [vmem] * 4,
        out_specs=(vmem, vmem),
        compiler_params=pltpu.CompilerParams(vmem_limit_bytes=16 * 1024 * 1024),
        name="carry",
    )(place, everyone, scale, shift, out_weight)

    quarter = half // 2
    even = [(0, 1), (1, 0), (2, 3), (3, 2)]
    odd = [(1, 2), (2, 1), (3, 0), (0, 3)]

    def added(mine, came):
        return (mine.astype(jnp.float32) + came.astype(jnp.float32)).astype(jnp.bfloat16)

    def summed(keep, send):
        came = swap_cores(send)
        low = added(keep[:quarter], came[:quarter])
        high = added(keep[quarter:], came[quarter:])
        low_came = lax.ppermute(low, "x", even)
        high_came = lax.ppermute(high, "x", odd)
        low = added(low, low_came)
        high = added(high, high_came)
        return low, lax.ppermute(low, "x", odd), high, lax.ppermute(high, "x", even)

    middle, near = pl.pallas_call(
        norm_body,
        out_shape=(half_shape, half_shape),
        in_specs=[smem] + [vmem] * 6,
        out_specs=(vmem, vmem),
        compiler_params=pltpu.CompilerParams(vmem_limit_bytes=16 * 1024 * 1024),
        name="norm",
    )(place, residual_in, *summed(keep, send), norm_gain.reshape(1, width))
    far = swap_cores(near)

    turns = len(left)
    span = width // turns
    blocks = [block for block, _ in left + right]
    plan = tuple(tuple(by for _, by in found) for found in (left, right))
    send, keep = pl.pallas_call(
        functools.partial(feed_body, plan),
        out_shape=(half_shape, half_shape),
        in_specs=[smem] + [vmem] * (2 + len(blocks)),
        out_specs=(vmem, vmem),
        scratch_shapes=[
            pltpu.VMEM((turns, length, span), jnp.bfloat16),
            pltpu.VMEM((turns, *right[0][0].shape), jnp.bfloat16),
            pltpu.VMEM((length, units + cut), jnp.float32),
            pltpu.VMEM((length, units), jnp.bfloat16),
        ],
        compiler_params=pltpu.CompilerParams(vmem_limit_bytes=28 * 1024 * 1024),
        name="feed",
    )(place, near, far, *(pltpu.with_memory_space_constraint(b, pltpu.VMEM) for b in blocks))
    low, low_came, high, high_came = summed(keep, send)

    def finished(rows, mine, came):
        channel_out = mine.astype(jnp.float32) + came.astype(jnp.float32)
        own = (rows.astype(jnp.float32) + channel_out).astype(jnp.bfloat16)
        return own, swap_cores(own)

    low, low_other = finished(middle[:quarter], low, low_came)
    high, high_other = finished(middle[quarter:], high, high_came)
    mine = (low, high)
    other = (low_other, high_other)
    first = [jnp.where(core == 0, a, b) for a, b in zip(mine, other)]
    last = [jnp.where(core == 0, b, a) for a, b in zip(mine, other)]
    return jnp.concatenate(first + last, axis=0)


def solution(mesh):
    sizes = (8, mesh.shape["sp"] // 8, mesh.shape["tp"] // 2, 2)
    torus = Mesh(mesh.devices.reshape(sizes), ("z", "y", "x", "core"))
    in_specs = (
        P(SP, None),
        P(TP, SP),
        P(TP, SP),
        P(TP, None),
        P(TP, None, None),
        P(TP, None, None),
        P(TP),
        P(TP, SP),
        P(TP, None),
        P(),
        P(SP, TP),
        P(SP, TP),
        P(SP, TP),
    )
    return jax.shard_map(
        on_device, mesh=torus, in_specs=in_specs, out_specs=P(SP, None), check_vma=False
    )
```

```python
import functools

import jax
import jax.numpy as jnp
import numpy as np
from jax import lax
from jax.experimental import pallas as pl
from jax.experimental.pallas import tpu as pltpu
from jax.sharding import Mesh
from jax.sharding import PartitionSpec as P

SP = ("z", "y")
TP = ("x", "core")
ALL = SP + TP


def shifted(value, by, fill):
    rows = value.shape[0]
    head = jnp.full((by, value.shape[1]), fill, value.dtype)
    if by % 8 == 0:
        return jnp.concatenate([head, value[: rows - by]], axis=0)
    rolled = pltpu.roll(value, by, 0)
    row = lax.broadcasted_iota(jnp.int32, value.shape, 0)
    return jnp.where(row < by, jnp.asarray(fill, value.dtype), rolled)


def recurrence_body(
    mixer, before, taps, recur, admit, rate, extra, branch, scale_out, shift_out, ends_out
):
    channels, length = mixer.shape
    tap_count = taps.shape[1]
    signal = mixer[...].astype(jnp.float32).T
    eye = (
        lax.broadcasted_iota(jnp.int32, (channels, channels), 0)
        == lax.broadcasted_iota(jnp.int32, (channels, channels), 1)
    ).astype(jnp.bfloat16)
    turn = (((0,), (0,)), ((), ()))
    tap_rows = lax.dot_general(taps[...], eye, turn, preferred_element_type=jnp.float32)
    halo = lax.dot_general(before[...], eye, turn, preferred_element_type=jnp.float32)
    row = lax.broadcasted_iota(jnp.int32, signal.shape, 0)
    conv_sum = jnp.zeros(signal.shape, jnp.float32)
    for tap in range(tap_count):
        back = tap_count - 1 - tap
        moved = signal
        if back:
            moved = pltpu.roll(signal, back, 0)
            for line in range(back):
                moved = jnp.where(row == line, halo[tap + line : tap + line + 1], moved)
        conv_sum = conv_sum + tap_rows[tap : tap + 1] * moved
    conv_out = conv_sum.astype(jnp.bfloat16)
    groups, width, _ = recur.shape
    spread = (
        lax.broadcasted_iota(jnp.int32, (width, channels), 1) % width
        == lax.broadcasted_iota(jnp.int32, (width, channels), 0)
    ).astype(jnp.bfloat16)
    same = (
        lax.broadcasted_iota(jnp.int32, (channels, channels), 0) // width
        == lax.broadcasted_iota(jnp.int32, (channels, channels), 1) // width
    )

    def gate(weight):
        flat = weight[...].reshape(groups * width, width)
        wide = jnp.dot(flat, spread, preferred_element_type=jnp.float32)
        wide = jnp.where(same, wide, 0.0).astype(jnp.bfloat16)
        return jax.nn.sigmoid(jnp.dot(conv_out, wide, preferred_element_type=jnp.float32))

    recur_gate = gate(recur)
    admit_gate = gate(admit)
    log_decay = -8.0 * recur_gate * rate[...] + extra[...].T
    run = jnp.exp(log_decay)
    twice = 2.0 * log_decay
    series = twice * (1.0 + twice * (0.5 + twice * (1.0 / 6.0 + twice * (1.0 / 24.0 + twice * (
        1.0 / 120.0 + twice * (1.0 / 720.0))))))
    lost = -jnp.where(twice > -0.25, series, run * run - 1.0)
    kept = jnp.where(lost > 0.0, jnp.sqrt(lost), 0.0)
    state = kept * admit_gate * conv_out.astype(jnp.float32)
    by = 1
    while by < length:
        state = state + run * shifted(state, by, 0.0)
        run = run * shifted(run, by, 1.0)
        by *= 2
    ends_out[0:1] = run[length - 1 : length]
    ends_out[1:2] = state[length - 1 : length]
    gelu = jax.nn.gelu(branch[...].astype(jnp.float32), approximate=True).T
    scale_out[...] = run * gelu
    shift_out[...] = state * gelu


def carry_body(place, ends, scale, shift, weight, send, keep):
    count = ends.shape[0]
    mine, core = place[0], place[1]
    half = send.shape[0]
    entering = jnp.zeros((1, scale.shape[1]), jnp.float32)
    for k in range(count):
        pair = ends[k]
        after = pair[0:1] * entering + pair[1:2]
        entering = jnp.where(k < mine, after, entering)
    for target, side in ((send, 1 - core), (keep, core)):
        at = pl.ds(pl.multiple_of(side * half, half), half)
        mixed = (shift[at, :] + scale[at, :] * entering).astype(jnp.bfloat16)
        found = jnp.dot(mixed, weight[...], preferred_element_type=jnp.float32)
        target[...] = found.astype(jnp.bfloat16)


def norm_body(place, residual, low, low_came, high, high_came, gain, middle, normed):
    half = middle.shape[0]
    quarter = half // 2
    for at, mine, came in ((0, low, low_came), (quarter, high, high_came)):
        branch = mine[...].astype(jnp.float32) + came[...].astype(jnp.float32)
        rows = pl.ds(pl.multiple_of(place[1] * half + at, quarter), quarter)
        found = (residual[rows, :].astype(jnp.float32) + branch).astype(jnp.bfloat16)
        middle[at : at + quarter, :] = found
        wide = found.astype(jnp.float32)
        row_scale = lax.rsqrt(jnp.mean(wide * wide, axis=1, keepdims=True) + 1e-06)
        ready = wide * row_scale * gain[...].astype(jnp.float32)
        normed[at : at + quarter, :] = ready.astype(jnp.bfloat16)


def feed_body(offsets, place, near, far, *refs):
    blocks = refs[: len(offsets)]
    send, keep, rows, stage, both_sum, hidden = refs[len(offsets) :]
    turns, length, span = rows.shape
    half = near.shape[0]
    units = hidden.shape[1]
    core, z, y = place[1], place[2], place[3]
    for k in range(turns):
        rows[k, :half] = near[:, k * span : (k + 1) * span]
        rows[k, half:] = far[:, k * span : (k + 1) * span]
    z_at = [lax.rem(z + (by + turns), turns) for by in offsets]
    y_at = [lax.rem(y + (by + turns), turns) for by in offsets]
    for outer, ref in enumerate(blocks):
        for inner in range(turns):
            row = jnp.where(core == 0, z_at[outer], z_at[inner])
            line = jnp.where(core == 0, y_at[inner], y_at[outer])
            stage[row, line] = ref[inner]
    total = None
    for k in range(turns):
        weight = stage[k, :, :, : 2 * units].reshape(span, 2 * units)
        part = jnp.dot(rows[k], weight, preferred_element_type=jnp.float32)
        if k % 2 == 0:
            total = part
        else:
            total = total + part
            if k == 1:
                both_sum[...] = total
            else:
                both_sum[...] += total
    gated = both_sum[:, :units]
    silu = gated / (1.0 + jnp.exp(-gated))
    hidden[...] = (silu * both_sum[:, units:]).astype(jnp.bfloat16)
    flip = (((1,), (1,)), ((), ()))
    for k in range(turns):
        down = stage[k, :, :, 2 * units :].reshape(span, units)
        found = lax.dot_general(hidden[...], down, flip, preferred_element_type=jnp.float32)
        keep[:, k * span : (k + 1) * span] = found[:half].astype(jnp.bfloat16)
        send[:, k * span : (k + 1) * span] = found[half:].astype(jnp.bfloat16)


def stack_body(*refs):
    out = refs[-1]
    for k, ref in enumerate(refs[:-1]):
        out[k] = ref[...]


def sent_to_all(value, axis):
    count = lax.axis_size(axis)
    return lax.all_to_all(
        jnp.broadcast_to(value[None], (count, *value.shape)), axis, 0, 0, tiled=True
    )


def moved(value, first, by):
    sizes = [lax.axis_size(axis) for axis in ALL]
    pairs = []
    for at in np.ndindex(*sizes):
        to = list(at)
        axis = first if at[3] == 0 else 1 - first
        to[axis] = (to[axis] + by) % sizes[axis]
        pairs.append((int(np.ravel_multi_index(at, sizes)), int(np.ravel_multi_index(to, sizes))))
    return lax.ppermute(value, ALL, pairs)


def both_ways(block, first, holds={}):
    found, ups, downs = [(block, 0)], block, block
    for k in range(1, 5):
        if k in holds:
            ups, downs, _ = lax.optimization_barrier((ups, downs, holds[k]))
        ups = moved(ups, first, 1)
        found.append((ups, -k))
        if k < 4:
            downs = moved(downs, first, -1)
            found.append((downs, k))
    return found


def swap_cores(value):
    return lax.ppermute(value, "core", [(0, 1), (1, 0)])


def on_device(
    residual_in,
    mixer_input,
    branch_gate,
    conv_taps,
    recur_weight,
    admit_weight,
    decay_param,
    decay_extra,
    out_weight,
    norm_gain,
    gate_weight,
    up_weight,
    down_weight,
):
    units = gate_weight.shape[1]
    smem = pl.BlockSpec(memory_space=pltpu.SMEM)
    vmem = pl.BlockSpec(memory_space=pltpu.VMEM)
    shard = jnp.concatenate([gate_weight, up_weight, down_weight], axis=1)
    channels, length = mixer_input.shape
    tap_count = conv_taps.shape[1]
    count = lax.axis_size(SP)
    tail = mixer_input[:, length - (tap_count - 1) :]
    before = lax.ppermute(tail, SP, [(i, i + 1) for i in range(count - 1)])
    square = jax.ShapeDtypeStruct((length, channels), jnp.float32)
    scale, shift, ends = pl.pallas_call(
        recurrence_body,
        out_shape=(square, square, jax.ShapeDtypeStruct((2, channels), jnp.float32)),
        in_specs=[pl.BlockSpec(memory_space=pltpu.VMEM)] * 8,
        out_specs=(pl.BlockSpec(memory_space=pltpu.VMEM),) * 3,
        compiler_params=pltpu.CompilerParams(vmem_limit_bytes=16 * 1024 * 1024),
        name="recurrence",
    )(
        mixer_input,
        before,
        conv_taps,
        recur_weight,
        admit_weight,
        jax.nn.softplus(-decay_param).reshape(1, channels),
        decay_extra,
        branch_gate,
    )
    everyone = sent_to_all(ends, SP)
    lines = both_ways(shard, 1, {2: before, 3: ends})
    lines = list(zip(lax.optimization_barrier((everyone, *(b for b, _ in lines)))[1:], [by for _, by in lines]))
    offsets = tuple(by for _, by in lines)
    block = pl.pallas_call(
        stack_body,
        out_shape=jax.ShapeDtypeStruct((len(lines), *shard.shape), shard.dtype),
        in_specs=[vmem] * len(lines),
        out_specs=vmem,
        compiler_params=pltpu.CompilerParams(vmem_limit_bytes=8 * 1024 * 1024),
        name="stack",
    )(*(pltpu.with_memory_space_constraint(b, pltpu.VMEM) for b, _ in lines))
    core = lax.axis_index("core")
    place = jnp.stack([lax.axis_index(SP), core, lax.axis_index("z"), lax.axis_index("y")])
    half = length // 2
    width = out_weight.shape[1]
    half_shape = jax.ShapeDtypeStruct((half, width), jnp.bfloat16)
    send, keep = pl.pallas_call(
        carry_body,
        out_shape=(half_shape, half_shape),
        in_specs=[smem] + [vmem] * 4,
        out_specs=(vmem, vmem),
        compiler_params=pltpu.CompilerParams(vmem_limit_bytes=16 * 1024 * 1024),
        name="carry",
    )(place, everyone, scale, shift, out_weight)

    quarter = half // 2
    even = [(0, 1), (1, 0), (2, 3), (3, 2)]
    odd = [(1, 2), (2, 1), (3, 0), (0, 3)]

    def added(mine, came):
        return (mine.astype(jnp.float32) + came.astype(jnp.float32)).astype(jnp.bfloat16)

    def paired(keep, send):
        came = swap_cores(send)
        return added(keep[:quarter], came[:quarter]), added(keep[quarter:], came[quarter:])

    def crossed(low, high):
        low_came = lax.ppermute(low, "x", even)
        high_came = lax.ppermute(high, "x", odd)
        low = added(low, low_came)
        high = added(high, high_came)
        return low, lax.ppermute(low, "x", odd), high, lax.ppermute(high, "x", even)

    paired_rows = paired(keep, send)
    crossed_rows = crossed(*paired_rows)
    holds = {2: paired_rows, 3: (crossed_rows[0], crossed_rows[2]), 4: crossed_rows[1]}
    blocks = [b for b, _ in both_ways(block, 0, holds)]
    middle, near = pl.pallas_call(
        norm_body,
        out_shape=(half_shape, half_shape),
        in_specs=[smem] + [vmem] * 6,
        out_specs=(vmem, vmem),
        compiler_params=pltpu.CompilerParams(vmem_limit_bytes=16 * 1024 * 1024),
        name="norm",
    )(place, residual_in, *crossed_rows, norm_gain.reshape(1, width))
    far = swap_cores(near)

    turns = len(blocks)
    send, keep = pl.pallas_call(
        functools.partial(feed_body, offsets),
        out_shape=(half_shape, half_shape),
        in_specs=[smem] + [vmem] * (2 + turns),
        out_specs=(vmem, vmem),
        scratch_shapes=[
            pltpu.VMEM((turns, length, width // turns), jnp.bfloat16),
            pltpu.VMEM((turns, *block.shape), jnp.bfloat16),
            pltpu.VMEM((length, 2 * units), jnp.float32),
            pltpu.VMEM((length, units), jnp.bfloat16),
        ],
        compiler_params=pltpu.CompilerParams(vmem_limit_bytes=28 * 1024 * 1024),
        name="feed",
    )(place, near, far, *(pltpu.with_memory_space_constraint(b, pltpu.VMEM) for b in blocks))
    low, low_came, high, high_came = crossed(*paired(keep, send))

    def finished(rows, mine, came):
        channel_out = mine.astype(jnp.float32) + came.astype(jnp.float32)
        own = (rows.astype(jnp.float32) + channel_out).astype(jnp.bfloat16)
        return own, swap_cores(own)

    low, low_other = finished(middle[:quarter], low, low_came)
    high_came, _ = lax.optimization_barrier((high_came, low))
    high, high_other = finished(middle[quarter:], high, high_came)
    mine = (low, high)
    other = (low_other, high_other)
    first = [jnp.where(core == 0, a, b) for a, b in zip(mine, other)]
    last = [jnp.where(core == 0, b, a) for a, b in zip(mine, other)]
    return jnp.concatenate(first + last, axis=0)


def solution(mesh):
    sizes = (8, mesh.shape["sp"] // 8, mesh.shape["tp"] // 2, 2)
    torus = Mesh(mesh.devices.reshape(sizes), ("z", "y", "x", "core"))
    in_specs = (
        P(SP, None),
        P(TP, SP),
        P(TP, SP),
        P(TP, None),
        P(TP, None, None),
        P(TP, None, None),
        P(TP),
        P(TP, SP),
        P(TP, None),
        P(),
        P(SP, TP),
        P(SP, TP),
        P(SP, TP),
    )
    return jax.shard_map(
        on_device, mesh=torus, in_specs=in_specs, out_specs=P(SP, None), check_vma=False
    )
```

```python
import jax
import jax.numpy as jnp
from jax import lax
from jax.experimental import pallas as pl
from jax.experimental.pallas import tpu as pltpu
from jax.sharding import Mesh
from jax.sharding import PartitionSpec as P

SP = ("z", "y")
TP = ("x", "core")


def shifted(value, by, fill):
    rows = value.shape[0]
    head = jnp.full((by, value.shape[1]), fill, value.dtype)
    if by % 8 == 0:
        return jnp.concatenate([head, value[: rows - by]], axis=0)
    rolled = pltpu.roll(value, by, 0)
    row = lax.broadcasted_iota(jnp.int32, value.shape, 0)
    return jnp.where(row < by, jnp.asarray(fill, value.dtype), rolled)


def recurrence_body(
    mixer, before, taps, recur, admit, rate, extra, branch, scale_out, shift_out, ends_out
):
    channels, length = mixer.shape
    tap_count = taps.shape[1]
    signal = mixer[...].astype(jnp.float32).T
    eye = (
        lax.broadcasted_iota(jnp.int32, (channels, channels), 0)
        == lax.broadcasted_iota(jnp.int32, (channels, channels), 1)
    ).astype(jnp.bfloat16)
    turn = (((0,), (0,)), ((), ()))
    tap_rows = lax.dot_general(taps[...], eye, turn, preferred_element_type=jnp.float32)
    halo = lax.dot_general(before[...], eye, turn, preferred_element_type=jnp.float32)
    row = lax.broadcasted_iota(jnp.int32, signal.shape, 0)
    conv_sum = jnp.zeros(signal.shape, jnp.float32)
    for tap in range(tap_count):
        back = tap_count - 1 - tap
        moved = signal
        if back:
            moved = pltpu.roll(signal, back, 0)
            for line in range(back):
                moved = jnp.where(row == line, halo[tap + line : tap + line + 1], moved)
        conv_sum = conv_sum + tap_rows[tap : tap + 1] * moved
    conv_out = conv_sum.astype(jnp.bfloat16)
    groups, width, _ = recur.shape
    spread = (
        lax.broadcasted_iota(jnp.int32, (width, channels), 1) % width
        == lax.broadcasted_iota(jnp.int32, (width, channels), 0)
    ).astype(jnp.bfloat16)
    same = (
        lax.broadcasted_iota(jnp.int32, (channels, channels), 0) // width
        == lax.broadcasted_iota(jnp.int32, (channels, channels), 1) // width
    )

    def gate(weight):
        flat = weight[...].reshape(groups * width, width)
        wide = jnp.dot(flat, spread, preferred_element_type=jnp.float32)
        wide = jnp.where(same, wide, 0.0).astype(jnp.bfloat16)
        return jax.nn.sigmoid(jnp.dot(conv_out, wide, preferred_element_type=jnp.float32))

    recur_gate = gate(recur)
    admit_gate = gate(admit)
    log_decay = -8.0 * recur_gate * rate[...] + extra[...].T
    run = jnp.exp(log_decay)
    twice = 2.0 * log_decay
    series = twice * (1.0 + twice * (0.5 + twice * (1.0 / 6.0 + twice * (1.0 / 24.0 + twice * (
        1.0 / 120.0 + twice * (1.0 / 720.0))))))
    lost = -jnp.where(twice > -0.25, series, run * run - 1.0)
    kept = jnp.where(lost > 0.0, jnp.sqrt(lost), 0.0)
    state = kept * admit_gate * conv_out.astype(jnp.float32)
    by = 1
    while by < length:
        state = state + run * shifted(state, by, 0.0)
        run = run * shifted(run, by, 1.0)
        by *= 2
    ends_out[0:1] = run[length - 1 : length]
    ends_out[1:2] = state[length - 1 : length]
    gelu = jax.nn.gelu(branch[...].astype(jnp.float32), approximate=True).T
    scale_out[...] = run * gelu
    shift_out[...] = state * gelu


def carry_body(place, ends, scale, shift, weight, send, keep):
    count = ends.shape[0]
    mine, core = place[0], place[1]
    half = send.shape[0]
    entering = jnp.zeros((1, scale.shape[1]), jnp.float32)
    for k in range(count):
        pair = ends[k]
        after = pair[0:1] * entering + pair[1:2]
        entering = jnp.where(k < mine, after, entering)
    for target, side in ((send, 1 - core), (keep, core)):
        at = pl.ds(pl.multiple_of(side * half, half), half)
        mixed = (shift[at, :] + scale[at, :] * entering).astype(jnp.bfloat16)
        found = jnp.dot(mixed, weight[...], preferred_element_type=jnp.float32)
        target[...] = found.astype(jnp.bfloat16)


def norm_body(place, residual, low, low_came, high, high_came, gain, middle, normed):
    half = middle.shape[0]
    quarter = half // 2
    for at, mine, came in ((0, low, low_came), (quarter, high, high_came)):
        branch = mine[...].astype(jnp.float32) + came[...].astype(jnp.float32)
        rows = pl.ds(pl.multiple_of(place[1] * half + at, quarter), quarter)
        found = (residual[rows, :].astype(jnp.float32) + branch).astype(jnp.bfloat16)
        middle[at : at + quarter, :] = found
        wide = found.astype(jnp.float32)
        row_scale = lax.rsqrt(jnp.mean(wide * wide, axis=1, keepdims=True) + 1e-06)
        ready = wide * row_scale * gain[...].astype(jnp.float32)
        normed[at : at + quarter, :] = ready.astype(jnp.bfloat16)


def feed_body(near, far, weights, send, keep, rows, stage, both_sum, hidden, arrived):
    parts, span, _ = stage.shape
    half = near.shape[0]
    units = hidden.shape[1]
    copies = [
        pltpu.make_async_copy(weights.at[pl.ds(k * span, span), :], stage.at[k], arrived.at[k])
        for k in range(parts)
    ]
    for copy in copies:
        copy.start()
    rows[:half] = near[...]
    rows[half:] = far[...]
    for k in range(0, parts, 2):
        found = None
        for piece in (k, k + 1):
            copies[piece].wait()
            part = jnp.dot(
                rows[:, piece * span : (piece + 1) * span],
                stage[piece, :, : 2 * units],
                preferred_element_type=jnp.float32,
            )
            found = part if found is None else found + part
        if k == 0:
            both_sum[...] = found
        else:
            both_sum[...] += found
    gated = both_sum[:, :units]
    silu = gated / (1.0 + jnp.exp(-gated))
    hidden[...] = (silu * both_sum[:, units:]).astype(jnp.bfloat16)
    flip = (((1,), (1,)), ((), ()))
    for k in range(parts):
        down = stage[k, :, 2 * units :]
        found = lax.dot_general(hidden[...], down, flip, preferred_element_type=jnp.float32)
        keep[:, k * span : (k + 1) * span] = found[:half].astype(jnp.bfloat16)
        send[:, k * span : (k + 1) * span] = found[half:].astype(jnp.bfloat16)


def swap_cores(value):
    return lax.ppermute(value, "core", [(0, 1), (1, 0)])


def on_device(
    residual_in,
    mixer_input,
    branch_gate,
    conv_taps,
    recur_weight,
    admit_weight,
    decay_param,
    decay_extra,
    out_weight,
    norm_gain,
    gate_weight,
    up_weight,
    down_weight,
):
    units = gate_weight.shape[1]
    weights = jnp.concatenate([gate_weight, up_weight, down_weight], axis=1)
    weights = lax.all_gather(weights, SP, axis=0, tiled=True)

    channels, length = mixer_input.shape
    tap_count = conv_taps.shape[1]
    count = lax.axis_size(SP)
    tail = mixer_input[:, length - (tap_count - 1) :]
    before = lax.ppermute(tail, SP, [(i, i + 1) for i in range(count - 1)])
    square = jax.ShapeDtypeStruct((length, channels), jnp.float32)
    scale, shift, ends = pl.pallas_call(
        recurrence_body,
        out_shape=(square, square, jax.ShapeDtypeStruct((2, channels), jnp.float32)),
        in_specs=[pl.BlockSpec(memory_space=pltpu.VMEM)] * 8,
        out_specs=(pl.BlockSpec(memory_space=pltpu.VMEM),) * 3,
        compiler_params=pltpu.CompilerParams(vmem_limit_bytes=16 * 1024 * 1024),
        name="recurrence",
    )(
        mixer_input,
        before,
        conv_taps,
        recur_weight,
        admit_weight,
        jax.nn.softplus(-decay_param).reshape(1, channels),
        decay_extra,
        branch_gate,
    )
    everyone = lax.all_to_all(
        jnp.broadcast_to(ends[None], (count, *ends.shape)), SP, 0, 0, tiled=True
    )
    core = lax.axis_index("core")
    place = jnp.stack([lax.axis_index(SP), core]).astype(jnp.int32)
    half = length // 2
    width = out_weight.shape[1]
    half_shape = jax.ShapeDtypeStruct((half, width), jnp.bfloat16)
    smem = pl.BlockSpec(memory_space=pltpu.SMEM)
    vmem = pl.BlockSpec(memory_space=pltpu.VMEM)
    send, keep = pl.pallas_call(
        carry_body,
        out_shape=(half_shape, half_shape),
        in_specs=[smem] + [vmem] * 4,
        out_specs=(vmem, vmem),
        compiler_params=pltpu.CompilerParams(vmem_limit_bytes=16 * 1024 * 1024),
        name="carry",
    )(place, everyone, scale, shift, out_weight)

    quarter = half // 2
    even = [(0, 1), (1, 0), (2, 3), (3, 2)]
    odd = [(1, 2), (2, 1), (3, 0), (0, 3)]

    def added(mine, came):
        return (mine.astype(jnp.float32) + came.astype(jnp.float32)).astype(jnp.bfloat16)

    def summed(keep, send):
        came = swap_cores(send)
        low = added(keep[:quarter], came[:quarter])
        high = added(keep[quarter:], came[quarter:])
        low_came = lax.ppermute(low, "x", even)
        high_came = lax.ppermute(high, "x", odd)
        low = added(low, low_came)
        high = added(high, high_came)
        return low, lax.ppermute(low, "x", odd), high, lax.ppermute(high, "x", even)

    middle, near = pl.pallas_call(
        norm_body,
        out_shape=(half_shape, half_shape),
        in_specs=[smem] + [vmem] * 6,
        out_specs=(vmem, vmem),
        compiler_params=pltpu.CompilerParams(vmem_limit_bytes=16 * 1024 * 1024),
        name="norm",
    )(place, residual_in, *summed(keep, send), norm_gain.reshape(1, width))
    far = swap_cores(near)

    parts = 8
    span = width // parts
    send, keep = pl.pallas_call(
        feed_body,
        out_shape=(half_shape, half_shape),
        in_specs=[vmem, vmem, pl.BlockSpec(memory_space=pl.ANY)],
        out_specs=(vmem, vmem),
        scratch_shapes=[
            pltpu.VMEM((length, width), jnp.bfloat16),
            pltpu.VMEM((parts, span, 3 * units), jnp.bfloat16),
            pltpu.VMEM((length, 2 * units), jnp.float32),
            pltpu.VMEM((length, units), jnp.bfloat16),
            pltpu.SemaphoreType.DMA((parts,)),
        ],
        compiler_params=pltpu.CompilerParams(vmem_limit_bytes=28 * 1024 * 1024),
        name="feed",
    )(
        pltpu.with_memory_space_constraint(near, pltpu.VMEM),
        pltpu.with_memory_space_constraint(far, pltpu.VMEM),
        pltpu.with_memory_space_constraint(weights, pltpu.HBM),
    )
    low, low_came, high, high_came = summed(keep, send)

    def finished(rows, mine, came):
        channel_out = mine.astype(jnp.float32) + came.astype(jnp.float32)
        own = (rows.astype(jnp.float32) + channel_out).astype(jnp.bfloat16)
        return own, swap_cores(own)

    low, low_other = finished(middle[:quarter], low, low_came)
    high_came, _ = lax.optimization_barrier((high_came, low))
    high, high_other = finished(middle[quarter:], high, high_came)
    mine = (low, high)
    other = (low_other, high_other)
    first = [jnp.where(core == 0, a, b) for a, b in zip(mine, other)]
    last = [jnp.where(core == 0, b, a) for a, b in zip(mine, other)]
    return jnp.concatenate(first + last, axis=0)


def solution(mesh):
    sizes = (8, mesh.shape["sp"] // 8, mesh.shape["tp"] // 2, 2)
    torus = Mesh(mesh.devices.reshape(sizes), ("z", "y", "x", "core"))
    in_specs = (
        P(SP, None),
        P(TP, SP),
        P(TP, SP),
        P(TP, None),
        P(TP, None, None),
        P(TP, None, None),
        P(TP),
        P(TP, SP),
        P(TP, None),
        P(),
        P(SP, TP),
        P(SP, TP),
        P(SP, TP),
    )
    return jax.shard_map(
        on_device, mesh=torus, in_specs=in_specs, out_specs=P(SP, None), check_vma=False
    )
```

```python
import jax
import jax.numpy as jnp
from jax import lax
from jax.experimental import pallas as pl
from jax.experimental.pallas import tpu as pltpu
from jax.sharding import Mesh
from jax.sharding import PartitionSpec as P

SP = ("z", "y")
TP = ("x", "core")


def shifted(value, by, fill):
    rows = value.shape[0]
    head = jnp.full((by, value.shape[1]), fill, value.dtype)
    if by % 8 == 0:
        return jnp.concatenate([head, value[: rows - by]], axis=0)
    rolled = pltpu.roll(value, by, 0)
    row = lax.broadcasted_iota(jnp.int32, value.shape, 0)
    return jnp.where(row < by, jnp.asarray(fill, value.dtype), rolled)


def recurrence_body(
    mixer, before, taps, recur, admit, rate, extra, branch, scale_out, shift_out, ends_out
):
    channels, length = mixer.shape
    tap_count = taps.shape[1]
    signal = mixer[...].astype(jnp.float32).T
    eye = (
        lax.broadcasted_iota(jnp.int32, (channels, channels), 0)
        == lax.broadcasted_iota(jnp.int32, (channels, channels), 1)
    ).astype(jnp.bfloat16)
    turn = (((0,), (0,)), ((), ()))
    tap_rows = lax.dot_general(taps[...], eye, turn, preferred_element_type=jnp.float32)
    halo = lax.dot_general(before[...], eye, turn, preferred_element_type=jnp.float32)
    row = lax.broadcasted_iota(jnp.int32, signal.shape, 0)
    conv_sum = jnp.zeros(signal.shape, jnp.float32)
    for tap in range(tap_count):
        back = tap_count - 1 - tap
        moved = signal
        if back:
            moved = pltpu.roll(signal, back, 0)
            for line in range(back):
                moved = jnp.where(row == line, halo[tap + line : tap + line + 1], moved)
        conv_sum = conv_sum + tap_rows[tap : tap + 1] * moved
    conv_out = conv_sum.astype(jnp.bfloat16)
    groups, width, _ = recur.shape
    spread = (
        lax.broadcasted_iota(jnp.int32, (width, channels), 1) % width
        == lax.broadcasted_iota(jnp.int32, (width, channels), 0)
    ).astype(jnp.bfloat16)
    same = (
        lax.broadcasted_iota(jnp.int32, (channels, channels), 0) // width
        == lax.broadcasted_iota(jnp.int32, (channels, channels), 1) // width
    )

    def gate(weight):
        flat = weight[...].reshape(groups * width, width)
        wide = jnp.dot(flat, spread, preferred_element_type=jnp.float32)
        wide = jnp.where(same, wide, 0.0).astype(jnp.bfloat16)
        return jax.nn.sigmoid(jnp.dot(conv_out, wide, preferred_element_type=jnp.float32))

    recur_gate = gate(recur)
    admit_gate = gate(admit)
    log_decay = -8.0 * recur_gate * rate[...] + extra[...].T
    run = jnp.exp(log_decay)
    twice = 2.0 * log_decay
    series = twice * (1.0 + twice * (0.5 + twice * (1.0 / 6.0 + twice * (1.0 / 24.0 + twice * (
        1.0 / 120.0 + twice * (1.0 / 720.0))))))
    lost = -jnp.where(twice > -0.25, series, run * run - 1.0)
    kept = jnp.where(lost > 0.0, jnp.sqrt(lost), 0.0)
    state = kept * admit_gate * conv_out.astype(jnp.float32)
    by = 1
    while by < length:
        state = state + run * shifted(state, by, 0.0)
        run = run * shifted(run, by, 1.0)
        by *= 2
    ends_out[0:1] = run[length - 1 : length]
    ends_out[1:2] = state[length - 1 : length]
    gelu = jax.nn.gelu(branch[...].astype(jnp.float32), approximate=True).T
    scale_out[...] = run * gelu
    shift_out[...] = state * gelu


def carry_body(place, ends, scale, shift, weight, send, keep):
    count = ends.shape[0]
    mine, core = place[0], place[1]
    half = send.shape[0]
    entering = jnp.zeros((1, scale.shape[1]), jnp.float32)
    for k in range(count):
        pair = ends[k]
        after = pair[0:1] * entering + pair[1:2]
        entering = jnp.where(k < mine, after, entering)
    for target, side in ((send, 1 - core), (keep, core)):
        at = pl.ds(pl.multiple_of(side * half, half), half)
        mixed = (shift[at, :] + scale[at, :] * entering).astype(jnp.bfloat16)
        found = jnp.dot(mixed, weight[...], preferred_element_type=jnp.float32)
        target[...] = found.astype(jnp.bfloat16)


def norm_body(place, residual, mine, came, gain, middle, normed):
    half = middle.shape[0]
    branch = mine[...].astype(jnp.float32) + came[...].astype(jnp.float32)
    rows = pl.ds(pl.multiple_of(place[1] * half, half), half)
    found = (residual[rows, :].astype(jnp.float32) + branch).astype(jnp.bfloat16)
    middle[...] = found
    wide = found.astype(jnp.float32)
    row_scale = lax.rsqrt(jnp.mean(wide * wide, axis=1, keepdims=True) + 1e-06)
    normed[...] = (wide * row_scale * gain[...].astype(jnp.float32)).astype(jnp.bfloat16)


def feed_body(near, far, weights, send, keep, rows, stage, down, both_sum, hidden, arrived):
    parts, span, wide = stage.shape
    blocks, depth, units = down.shape
    half = near.shape[0]
    copies = [
        pltpu.make_async_copy(
            weights.at[pl.ds(k * span, span), pl.ds(0, wide)], stage.at[k], arrived.at[k]
        )
        for k in range(parts)
    ]
    copies += [
        pltpu.make_async_copy(
            weights.at[pl.ds(k * depth, depth), pl.ds(wide, units)],
            down.at[k],
            arrived.at[parts + k],
        )
        for k in range(blocks)
    ]
    for copy in copies:
        copy.start()
    rows[:half] = near[...]
    rows[half:] = far[...]
    for k in range(0, parts, 2):
        found = None
        for piece in (k, k + 1):
            copies[piece].wait()
            part = jnp.dot(
                rows[:, piece * span : (piece + 1) * span],
                stage[piece],
                preferred_element_type=jnp.float32,
            )
            found = part if found is None else found + part
        if k == 0:
            both_sum[...] = found
        else:
            both_sum[...] += found
    gated = both_sum[:, :units]
    silu = gated / (1.0 + jnp.exp(-gated))
    hidden[...] = (silu * both_sum[:, units:]).astype(jnp.bfloat16)
    flip = (((1,), (1,)), ((), ()))
    for k in range(blocks):
        copies[parts + k].wait()
        found = lax.dot_general(hidden[...], down[k], flip, preferred_element_type=jnp.float32)
        keep[:, k * depth : (k + 1) * depth] = found[:half].astype(jnp.bfloat16)
        send[:, k * depth : (k + 1) * depth] = found[half:].astype(jnp.bfloat16)


def swap_cores(value):
    return lax.ppermute(value, "core", [(0, 1), (1, 0)])


def on_device(
    residual_in,
    mixer_input,
    branch_gate,
    conv_taps,
    recur_weight,
    admit_weight,
    decay_param,
    decay_extra,
    out_weight,
    norm_gain,
    gate_weight,
    up_weight,
    down_weight,
):
    units = gate_weight.shape[1]
    weights = jnp.concatenate([gate_weight, up_weight, down_weight], axis=1)
    weights = lax.all_gather(weights, SP, axis=0, tiled=True)

    channels, length = mixer_input.shape
    tap_count = conv_taps.shape[1]
    count = lax.axis_size(SP)
    tail = mixer_input[:, length - (tap_count - 1) :]
    before = lax.ppermute(tail, SP, [(i, i + 1) for i in range(count - 1)])
    square = jax.ShapeDtypeStruct((length, channels), jnp.float32)
    scale, shift, ends = pl.pallas_call(
        recurrence_body,
        out_shape=(square, square, jax.ShapeDtypeStruct((2, channels), jnp.float32)),
        in_specs=[pl.BlockSpec(memory_space=pltpu.VMEM)] * 8,
        out_specs=(pl.BlockSpec(memory_space=pltpu.VMEM),) * 3,
        compiler_params=pltpu.CompilerParams(vmem_limit_bytes=16 * 1024 * 1024),
        name="recurrence",
    )(
        mixer_input,
        before,
        conv_taps,
        recur_weight,
        admit_weight,
        jax.nn.softplus(-decay_param).reshape(1, channels),
        decay_extra,
        branch_gate,
    )
    everyone = lax.all_to_all(
        jnp.broadcast_to(ends[None], (count, *ends.shape)), SP, 0, 0, tiled=True
    )
    core = lax.axis_index("core")
    place = jnp.stack([lax.axis_index(SP), core]).astype(jnp.int32)
    half = length // 2
    width = out_weight.shape[1]
    half_shape = jax.ShapeDtypeStruct((half, width), jnp.bfloat16)
    smem = pl.BlockSpec(memory_space=pltpu.SMEM)
    vmem = pl.BlockSpec(memory_space=pltpu.VMEM)
    send, keep = pl.pallas_call(
        carry_body,
        out_shape=(half_shape, half_shape),
        in_specs=[smem] + [vmem] * 4,
        out_specs=(vmem, vmem),
        compiler_params=pltpu.CompilerParams(vmem_limit_bytes=16 * 1024 * 1024),
        name="carry",
    )(place, everyone, scale, shift, out_weight)

    even, odd = (1, 0, 3, 2), (3, 2, 1, 0)

    def added(mine, came):
        return (mine.astype(jnp.float32) + came.astype(jnp.float32)).astype(jnp.bfloat16)

    def paired(value, by_core):
        pairs = [(2 * x + c, 2 * by_core[c][x] + c) for x in range(4) for c in range(2)]
        return lax.ppermute(value, TP, pairs)

    def summed(keep, send):
        mine = added(keep, swap_cores(send))
        mine = added(mine, paired(mine, (even, odd)))
        return mine, paired(mine, (odd, even))

    middle, near = pl.pallas_call(
        norm_body,
        out_shape=(half_shape, half_shape),
        in_specs=[smem] + [vmem] * 4,
        out_specs=(vmem, vmem),
        compiler_params=pltpu.CompilerParams(vmem_limit_bytes=16 * 1024 * 1024),
        name="norm",
    )(place, residual_in, *summed(keep, send), norm_gain.reshape(1, width))
    far = swap_cores(near)

    parts = 8
    span = width // parts
    send, keep = pl.pallas_call(
        feed_body,
        out_shape=(half_shape, half_shape),
        in_specs=[vmem, vmem, pl.BlockSpec(memory_space=pl.ANY)],
        out_specs=(vmem, vmem),
        scratch_shapes=[
            pltpu.VMEM((length, width), jnp.bfloat16),
            pltpu.VMEM((parts, span, 2 * units), jnp.bfloat16),
            pltpu.VMEM((4, width // 4, units), jnp.bfloat16),
            pltpu.VMEM((length, 2 * units), jnp.float32),
            pltpu.VMEM((length, units), jnp.bfloat16),
            pltpu.SemaphoreType.DMA((parts + 4,)),
        ],
        compiler_params=pltpu.CompilerParams(vmem_limit_bytes=28 * 1024 * 1024),
        name="feed",
    )(
        pltpu.with_memory_space_constraint(near, pltpu.VMEM),
        pltpu.with_memory_space_constraint(far, pltpu.VMEM),
        pltpu.with_memory_space_constraint(weights, pltpu.HBM),
    )
    mine, came = summed(keep, send)
    channel_out = mine.astype(jnp.float32) + came.astype(jnp.float32)
    mine = (middle.astype(jnp.float32) + channel_out).astype(jnp.bfloat16)
    other = swap_cores(mine)
    first = jnp.where(core == 0, mine, other)
    last = jnp.where(core == 0, other, mine)
    return jnp.concatenate([first, last], axis=0)


def solution(mesh):
    sizes = (8, mesh.shape["sp"] // 8, mesh.shape["tp"] // 2, 2)
    torus = Mesh(mesh.devices.reshape(sizes), ("z", "y", "x", "core"))
    in_specs = (
        P(SP, None),
        P(TP, SP),
        P(TP, SP),
        P(TP, None),
        P(TP, None, None),
        P(TP, None, None),
        P(TP),
        P(TP, SP),
        P(TP, None),
        P(),
        P(SP, TP),
        P(SP, TP),
        P(SP, TP),
    )
    return jax.shard_map(
        on_device, mesh=torus, in_specs=in_specs, out_specs=P(SP, None), check_vma=False
    )
```

```python
import jax
import jax.numpy as jnp
from jax import lax
from jax.experimental import pallas as pl
from jax.experimental.pallas import tpu as pltpu
from jax.sharding import Mesh
from jax.sharding import PartitionSpec as P

SP = ("z", "y")
TP = ("x", "core")


def shifted(value, by, fill):
    rows = value.shape[0]
    head = jnp.full((by, value.shape[1]), fill, value.dtype)
    if by % 8 == 0:
        return jnp.concatenate([head, value[: rows - by]], axis=0)
    rolled = pltpu.roll(value, by, 0)
    row = lax.broadcasted_iota(jnp.int32, value.shape, 0)
    return jnp.where(row < by, jnp.asarray(fill, value.dtype), rolled)


def recurrence_body(
    mixer, before, taps, recur, admit, rate, extra, branch, scale_out, shift_out, ends_out
):
    channels, length = mixer.shape
    tap_count = taps.shape[1]
    signal = mixer[...].astype(jnp.float32).T
    eye = (
        lax.broadcasted_iota(jnp.int32, (channels, channels), 0)
        == lax.broadcasted_iota(jnp.int32, (channels, channels), 1)
    ).astype(jnp.bfloat16)
    turn = (((0,), (0,)), ((), ()))
    tap_rows = lax.dot_general(taps[...], eye, turn, preferred_element_type=jnp.float32)
    halo = lax.dot_general(before[...], eye, turn, preferred_element_type=jnp.float32)
    row = lax.broadcasted_iota(jnp.int32, signal.shape, 0)
    conv_sum = jnp.zeros(signal.shape, jnp.float32)
    for tap in range(tap_count):
        back = tap_count - 1 - tap
        moved = signal
        if back:
            moved = pltpu.roll(signal, back, 0)
            for line in range(back):
                moved = jnp.where(row == line, halo[tap + line : tap + line + 1], moved)
        conv_sum = conv_sum + tap_rows[tap : tap + 1] * moved
    conv_out = conv_sum.astype(jnp.bfloat16)
    groups, width, _ = recur.shape
    spread = (
        lax.broadcasted_iota(jnp.int32, (width, channels), 1) % width
        == lax.broadcasted_iota(jnp.int32, (width, channels), 0)
    ).astype(jnp.bfloat16)
    same = (
        lax.broadcasted_iota(jnp.int32, (channels, channels), 0) // width
        == lax.broadcasted_iota(jnp.int32, (channels, channels), 1) // width
    )

    def gate(weight):
        flat = weight[...].reshape(groups * width, width)
        wide = jnp.dot(flat, spread, preferred_element_type=jnp.float32)
        wide = jnp.where(same, wide, 0.0).astype(jnp.bfloat16)
        return jax.nn.sigmoid(jnp.dot(conv_out, wide, preferred_element_type=jnp.float32))

    recur_gate = gate(recur)
    admit_gate = gate(admit)
    log_decay = -8.0 * recur_gate * rate[...] + extra[...].T
    run = jnp.exp(log_decay)
    twice = 2.0 * log_decay
    series = twice * (1.0 + twice * (0.5 + twice * (1.0 / 6.0 + twice * (1.0 / 24.0 + twice * (
        1.0 / 120.0 + twice * (1.0 / 720.0))))))
    lost = -jnp.where(twice > -0.25, series, run * run - 1.0)
    kept = jnp.where(lost > 0.0, jnp.sqrt(lost), 0.0)
    state = kept * admit_gate * conv_out.astype(jnp.float32)
    by = 1
    while by < length:
        state = state + run * shifted(state, by, 0.0)
        run = run * shifted(run, by, 1.0)
        by *= 2
    ends_out[0:1] = run[length - 1 : length]
    ends_out[1:2] = state[length - 1 : length]
    gelu = jax.nn.gelu(branch[...].astype(jnp.float32), approximate=True).T
    scale_out[...] = run * gelu
    shift_out[...] = state * gelu


def folded(pairs, limit, scale, shift):
    for k in range(pairs.shape[0]):
        pair = pairs[k]
        after_scale, after_shift = pair[0:1] * scale, pair[0:1] * shift + pair[1:2]
        scale = jnp.where(k < limit, after_scale, scale)
        shift = jnp.where(k < limit, after_shift, shift)
    return scale, shift


def combine_body(place, line, before, total):
    one = jnp.ones((1, line.shape[2]), jnp.float32)
    for target, limit in ((before, place[0]), (total, line.shape[0])):
        scale, shift = folded(line, limit, one, 0.0 * one)
        target[0:1] = scale
        target[1:2] = shift


def carry_body(place, rows, before, scale, shift, weight, send, keep):
    core, z = place[1], place[2]
    half = send.shape[0]
    one = jnp.ones((1, scale.shape[1]), jnp.float32)
    entering = folded(rows, z, one, 0.0 * one)[1]
    entering = before[0:1] * entering + before[1:2]
    for target, side in ((send, 1 - core), (keep, core)):
        at = pl.ds(pl.multiple_of(side * half, half), half)
        mixed = (shift[at, :] + scale[at, :] * entering).astype(jnp.bfloat16)
        found = jnp.dot(mixed, weight[...], preferred_element_type=jnp.float32)
        target[...] = found.astype(jnp.bfloat16)


def norm_body(place, residual, mine, came, gain, middle, normed):
    half = middle.shape[0]
    branch = mine[...].astype(jnp.float32) + came[...].astype(jnp.float32)
    rows = pl.ds(pl.multiple_of(place[1] * half, half), half)
    found = (residual[rows, :].astype(jnp.float32) + branch).astype(jnp.bfloat16)
    middle[...] = found
    wide = found.astype(jnp.float32)
    row_scale = lax.rsqrt(jnp.mean(wide * wide, axis=1, keepdims=True) + 1e-06)
    normed[...] = (wide * row_scale * gain[...].astype(jnp.float32)).astype(jnp.bfloat16)


def feed_body(near, far, weights, send, keep, rows, stage, both_sum, hidden, arrived):
    parts, span, _ = stage.shape
    half = near.shape[0]
    units = hidden.shape[1]
    copies = [
        pltpu.make_async_copy(weights.at[pl.ds(k * span, span), :], stage.at[k], arrived.at[k])
        for k in range(parts)
    ]
    for copy in copies:
        copy.start()
    rows[:half] = near[...]
    rows[half:] = far[...]
    for k in range(0, parts, 2):
        found = None
        for piece in (k, k + 1):
            copies[piece].wait()
            part = jnp.dot(
                rows[:, piece * span : (piece + 1) * span],
                stage[piece, :, : 2 * units],
                preferred_element_type=jnp.float32,
            )
            found = part if found is None else found + part
        if k == 0:
            both_sum[...] = found
        else:
            both_sum[...] += found
    gated = both_sum[:, :units]
    silu = gated / (1.0 + jnp.exp(-gated))
    hidden[...] = (silu * both_sum[:, units:]).astype(jnp.bfloat16)
    flip = (((1,), (1,)), ((), ()))
    for k in range(parts):
        down = stage[k, :, 2 * units :]
        found = lax.dot_general(hidden[...], down, flip, preferred_element_type=jnp.float32)
        keep[:, k * span : (k + 1) * span] = found[:half].astype(jnp.bfloat16)
        send[:, k * span : (k + 1) * span] = found[half:].astype(jnp.bfloat16)


def sent_to_all(value, axis):
    count = lax.axis_size(axis)
    return lax.all_to_all(
        jnp.broadcast_to(value[None], (count, *value.shape)), axis, 0, 0, tiled=True
    )


def swap_cores(value):
    return lax.ppermute(value, "core", [(0, 1), (1, 0)])


def on_device(
    residual_in,
    mixer_input,
    branch_gate,
    conv_taps,
    recur_weight,
    admit_weight,
    decay_param,
    decay_extra,
    out_weight,
    norm_gain,
    gate_weight,
    up_weight,
    down_weight,
):
    units = gate_weight.shape[1]
    weights = jnp.concatenate([gate_weight, up_weight, down_weight], axis=1)
    weights = lax.all_gather(weights, SP, axis=0, tiled=True)

    channels, length = mixer_input.shape
    tap_count = conv_taps.shape[1]
    count = lax.axis_size(SP)
    tail = mixer_input[:, length - (tap_count - 1) :]
    before = lax.ppermute(tail, SP, [(i, i + 1) for i in range(count - 1)])
    square = jax.ShapeDtypeStruct((length, channels), jnp.float32)
    scale, shift, ends = pl.pallas_call(
        recurrence_body,
        out_shape=(square, square, jax.ShapeDtypeStruct((2, channels), jnp.float32)),
        in_specs=[pl.BlockSpec(memory_space=pltpu.VMEM)] * 8,
        out_specs=(pl.BlockSpec(memory_space=pltpu.VMEM),) * 3,
        compiler_params=pltpu.CompilerParams(vmem_limit_bytes=16 * 1024 * 1024),
        name="recurrence",
    )(
        mixer_input,
        before,
        conv_taps,
        recur_weight,
        admit_weight,
        jax.nn.softplus(-decay_param).reshape(1, channels),
        decay_extra,
        branch_gate,
    )
    smem = pl.BlockSpec(memory_space=pltpu.SMEM)
    vmem = pl.BlockSpec(memory_space=pltpu.VMEM)
    y_place = lax.axis_index("y").astype(jnp.int32).reshape(1)
    pair_shape = jax.ShapeDtypeStruct(ends.shape, jnp.float32)
    earlier, total = pl.pallas_call(
        combine_body,
        out_shape=(pair_shape, pair_shape),
        in_specs=[smem, vmem],
        out_specs=(vmem, vmem),
        compiler_params=pltpu.CompilerParams(vmem_limit_bytes=8 * 1024 * 1024),
        name="combine",
    )(y_place, sent_to_all(ends, "y"))
    everyone = sent_to_all(total, "z")
    core = lax.axis_index("core")
    place = jnp.stack([lax.axis_index(SP), core, lax.axis_index("z")]).astype(jnp.int32)
    half = length // 2
    width = out_weight.shape[1]
    half_shape = jax.ShapeDtypeStruct((half, width), jnp.bfloat16)
    send, keep = pl.pallas_call(
        carry_body,
        out_shape=(half_shape, half_shape),
        in_specs=[smem] + [vmem] * 5,
        out_specs=(vmem, vmem),
        compiler_params=pltpu.CompilerParams(vmem_limit_bytes=16 * 1024 * 1024),
        name="carry",
    )(place, everyone, earlier, scale, shift, out_weight)

    even, odd = (1, 0, 3, 2), (3, 2, 1, 0)

    def added(mine, came):
        return (mine.astype(jnp.float32) + came.astype(jnp.float32)).astype(jnp.bfloat16)

    def paired(value, by_core):
        pairs = [(2 * x + c, 2 * by_core[c][x] + c) for x in range(4) for c in range(2)]
        return lax.ppermute(value, TP, pairs)

    def summed(keep, send):
        mine = added(keep, swap_cores(send))
        mine = added(mine, paired(mine, (even, odd)))
        return mine, paired(mine, (odd, even))

    middle, near = pl.pallas_call(
        norm_body,
        out_shape=(half_shape, half_shape),
        in_specs=[smem] + [vmem] * 4,
        out_specs=(vmem, vmem),
        compiler_params=pltpu.CompilerParams(vmem_limit_bytes=16 * 1024 * 1024),
        name="norm",
    )(place, residual_in, *summed(keep, send), norm_gain.reshape(1, width))
    far = swap_cores(near)

    parts = 8
    span = width // parts
    send, keep = pl.pallas_call(
        feed_body,
        out_shape=(half_shape, half_shape),
        in_specs=[vmem, vmem, pl.BlockSpec(memory_space=pl.ANY)],
        out_specs=(vmem, vmem),
        scratch_shapes=[
            pltpu.VMEM((length, width), jnp.bfloat16),
            pltpu.VMEM((parts, span, 3 * units), jnp.bfloat16),
            pltpu.VMEM((length, 2 * units), jnp.float32),
            pltpu.VMEM((length, units), jnp.bfloat16),
            pltpu.SemaphoreType.DMA((parts,)),
        ],
        compiler_params=pltpu.CompilerParams(vmem_limit_bytes=28 * 1024 * 1024),
        name="feed",
    )(
        pltpu.with_memory_space_constraint(near, pltpu.VMEM),
        pltpu.with_memory_space_constraint(far, pltpu.VMEM),
        pltpu.with_memory_space_constraint(weights, pltpu.HBM),
    )
    mine, came = summed(keep, send)
    channel_out = mine.astype(jnp.float32) + came.astype(jnp.float32)
    mine = (middle.astype(jnp.float32) + channel_out).astype(jnp.bfloat16)
    other = swap_cores(mine)
    first = jnp.where(core == 0, mine, other)
    last = jnp.where(core == 0, other, mine)
    return jnp.concatenate([first, last], axis=0)


def solution(mesh):
    sizes = (8, mesh.shape["sp"] // 8, mesh.shape["tp"] // 2, 2)
    torus = Mesh(mesh.devices.reshape(sizes), ("z", "y", "x", "core"))
    in_specs = (
        P(SP, None),
        P(TP, SP),
        P(TP, SP),
        P(TP, None),
        P(TP, None, None),
        P(TP, None, None),
        P(TP),
        P(TP, SP),
        P(TP, None),
        P(),
        P(SP, TP),
        P(SP, TP),
        P(SP, TP),
    )
    return jax.shard_map(
        on_device, mesh=torus, in_specs=in_specs, out_specs=P(SP, None), check_vma=False
    )
```

```python
import functools

import jax
import jax.numpy as jnp
from jax import lax
from jax.experimental import pallas as pl
from jax.experimental.pallas import tpu as pltpu
from jax.sharding import Mesh
from jax.sharding import PartitionSpec as P

SP = ("z", "y")
TP = ("x", "core")


def shifted(value, by, fill):
    rows = value.shape[0]
    head = jnp.full((by, value.shape[1]), fill, value.dtype)
    if by % 8 == 0:
        return jnp.concatenate([head, value[: rows - by]], axis=0)
    rolled = pltpu.roll(value, by, 0)
    row = lax.broadcasted_iota(jnp.int32, value.shape, 0)
    return jnp.where(row < by, jnp.asarray(fill, value.dtype), rolled)


def recurrence_body(
    mixer, before, taps, recur, admit, rate, extra, branch, scale_out, shift_out, ends_out
):
    channels, length = mixer.shape
    tap_count = taps.shape[1]
    signal = mixer[...].astype(jnp.float32).T
    eye = (
        lax.broadcasted_iota(jnp.int32, (channels, channels), 0)
        == lax.broadcasted_iota(jnp.int32, (channels, channels), 1)
    ).astype(jnp.bfloat16)
    turn = (((0,), (0,)), ((), ()))
    tap_rows = lax.dot_general(taps[...], eye, turn, preferred_element_type=jnp.float32)
    halo = lax.dot_general(before[...], eye, turn, preferred_element_type=jnp.float32)
    row = lax.broadcasted_iota(jnp.int32, signal.shape, 0)
    conv_sum = jnp.zeros(signal.shape, jnp.float32)
    for tap in range(tap_count):
        back = tap_count - 1 - tap
        moved = signal
        if back:
            moved = pltpu.roll(signal, back, 0)
            for line in range(back):
                moved = jnp.where(row == line, halo[tap + line : tap + line + 1], moved)
        conv_sum = conv_sum + tap_rows[tap : tap + 1] * moved
    conv_out = conv_sum.astype(jnp.bfloat16)
    groups, width, _ = recur.shape
    spread = (
        lax.broadcasted_iota(jnp.int32, (width, channels), 1) % width
        == lax.broadcasted_iota(jnp.int32, (width, channels), 0)
    ).astype(jnp.bfloat16)
    same = (
        lax.broadcasted_iota(jnp.int32, (channels, channels), 0) // width
        == lax.broadcasted_iota(jnp.int32, (channels, channels), 1) // width
    )

    def gate(weight):
        flat = weight[...].reshape(groups * width, width)
        wide = jnp.dot(flat, spread, preferred_element_type=jnp.float32)
        wide = jnp.where(same, wide, 0.0).astype(jnp.bfloat16)
        return jax.nn.sigmoid(jnp.dot(conv_out, wide, preferred_element_type=jnp.float32))

    recur_gate = gate(recur)
    admit_gate = gate(admit)
    log_decay = -8.0 * recur_gate * rate[...] + extra[...].T
    run = jnp.exp(log_decay)
    twice = 2.0 * log_decay
    series = twice * (1.0 + twice * (0.5 + twice * (1.0 / 6.0 + twice * (1.0 / 24.0 + twice * (
        1.0 / 120.0 + twice * (1.0 / 720.0))))))
    lost = -jnp.where(twice > -0.25, series, run * run - 1.0)
    kept = jnp.where(lost > 0.0, jnp.sqrt(lost), 0.0)
    state = kept * admit_gate * conv_out.astype(jnp.float32)
    by = 1
    while by < length:
        state = state + run * shifted(state, by, 0.0)
        run = run * shifted(run, by, 1.0)
        by *= 2
    ends_out[0:1] = run[length - 1 : length]
    ends_out[1:2] = state[length - 1 : length]
    gelu = jax.nn.gelu(branch[...].astype(jnp.float32), approximate=True).T
    scale_out[...] = run * gelu
    shift_out[...] = state * gelu


def folded(pairs, limit, scale, shift):
    for k in range(pairs.shape[0]):
        pair = pairs[k]
        after_scale, after_shift = pair[0:1] * scale, pair[0:1] * shift + pair[1:2]
        scale = jnp.where(k < limit, after_scale, scale)
        shift = jnp.where(k < limit, after_shift, shift)
    return scale, shift


def combine_body(place, line, before, total):
    one = jnp.ones((1, line.shape[2]), jnp.float32)
    for target, limit in ((before, place[0]), (total, line.shape[0])):
        scale, shift = folded(line, limit, one, 0.0 * one)
        target[0:1] = scale
        target[1:2] = shift


def carry_body(place, rows, before, scale, shift, weight, send, keep):
    core, z = place[1], place[2]
    half = send.shape[0]
    one = jnp.ones((1, scale.shape[1]), jnp.float32)
    entering = folded(rows, z, one, 0.0 * one)[1]
    entering = before[0:1] * entering + before[1:2]
    for target, side in ((send, 1 - core), (keep, core)):
        at = pl.ds(pl.multiple_of(side * half, half), half)
        mixed = (shift[at, :] + scale[at, :] * entering).astype(jnp.bfloat16)
        found = jnp.dot(mixed, weight[...], preferred_element_type=jnp.float32)
        target[...] = found.astype(jnp.bfloat16)


def norm_body(place, residual, low, low_came, high, high_came, gain, middle, normed):
    half = middle.shape[0]
    quarter = half // 2
    for at, mine, came in ((0, low, low_came), (quarter, high, high_came)):
        branch = mine[...].astype(jnp.float32) + came[...].astype(jnp.float32)
        rows = pl.ds(pl.multiple_of(place[1] * half + at, quarter), quarter)
        found = (residual[rows, :].astype(jnp.float32) + branch).astype(jnp.bfloat16)
        middle[at : at + quarter, :] = found
        wide = found.astype(jnp.float32)
        row_scale = lax.rsqrt(jnp.mean(wide * wide, axis=1, keepdims=True) + 1e-06)
        ready = wide * row_scale * gain[...].astype(jnp.float32)
        normed[at : at + quarter, :] = ready.astype(jnp.bfloat16)


def finish_body(middle, low, low_came, high, high_came, out):
    quarter = low.shape[0]
    for at, mine, came in ((0, low, low_came), (quarter, high, high_came)):
        rows = pl.ds(at, quarter)
        channel_out = mine[...].astype(jnp.float32) + came[...].astype(jnp.float32)
        out[rows, :] = (middle[rows, :].astype(jnp.float32) + channel_out).astype(jnp.bfloat16)


def write_body(side, place, value, *refs):
    out, done = refs[-2:]
    half = value.shape[0]
    at = pl.multiple_of((place[1] if side == 0 else 1 - place[1]) * half, half)
    copy = pltpu.make_async_copy(value, out.at[pl.ds(at, half), :], done)
    copy.start()
    copy.wait()


def feed_body(near, far, weights, send, keep, rows, stage, both_sum, hidden, arrived):
    parts, span, _ = stage.shape
    half = near.shape[0]
    units = hidden.shape[1]
    copies = [
        pltpu.make_async_copy(weights.at[pl.ds(k * span, span), :], stage.at[k], arrived.at[k])
        for k in range(parts)
    ]
    for copy in copies:
        copy.start()
    rows[:half] = near[...]
    rows[half:] = far[...]
    for k in range(0, parts, 2):
        found = None
        for piece in (k, k + 1):
            copies[piece].wait()
            part = jnp.dot(
                rows[:, piece * span : (piece + 1) * span],
                stage[piece, :, : 2 * units],
                preferred_element_type=jnp.float32,
            )
            found = part if found is None else found + part
        if k == 0:
            both_sum[...] = found
        else:
            both_sum[...] += found
    gated = both_sum[:, :units]
    silu = gated / (1.0 + jnp.exp(-gated))
    hidden[...] = (silu * both_sum[:, units:]).astype(jnp.bfloat16)
    flip = (((1,), (1,)), ((), ()))
    for k in range(parts):
        down = stage[k, :, 2 * units :]
        found = lax.dot_general(hidden[...], down, flip, preferred_element_type=jnp.float32)
        keep[:, k * span : (k + 1) * span] = found[:half].astype(jnp.bfloat16)
        send[:, k * span : (k + 1) * span] = found[half:].astype(jnp.bfloat16)


def sent_to_all(value, axis):
    count = lax.axis_size(axis)
    return lax.all_to_all(
        jnp.broadcast_to(value[None], (count, *value.shape)), axis, 0, 0, tiled=True
    )


def stays(value):
    return pltpu.with_memory_space_constraint(value, pltpu.VMEM)


def swap_cores(value):
    return lax.ppermute(value, "core", [(0, 1), (1, 0)])


def on_device(
    residual_in,
    mixer_input,
    branch_gate,
    conv_taps,
    recur_weight,
    admit_weight,
    decay_param,
    decay_extra,
    out_weight,
    norm_gain,
    gate_weight,
    up_weight,
    down_weight,
):
    units = gate_weight.shape[1]
    weights = jnp.concatenate([gate_weight, up_weight, down_weight], axis=1)
    weights = lax.all_gather(weights, SP, axis=0, tiled=True)

    channels, length = mixer_input.shape
    tap_count = conv_taps.shape[1]
    count = lax.axis_size(SP)
    tail = mixer_input[:, length - (tap_count - 1) :]
    before = lax.ppermute(tail, SP, [(i, i + 1) for i in range(count - 1)])
    square = jax.ShapeDtypeStruct((length, channels), jnp.float32)
    scale, shift, ends = pl.pallas_call(
        recurrence_body,
        out_shape=(square, square, jax.ShapeDtypeStruct((2, channels), jnp.float32)),
        in_specs=[pl.BlockSpec(memory_space=pltpu.VMEM)] * 8,
        out_specs=(pl.BlockSpec(memory_space=pltpu.VMEM),) * 3,
        compiler_params=pltpu.CompilerParams(vmem_limit_bytes=16 * 1024 * 1024),
        name="recurrence",
    )(
        mixer_input,
        before,
        conv_taps,
        recur_weight,
        admit_weight,
        jax.nn.softplus(-decay_param).reshape(1, channels),
        decay_extra,
        branch_gate,
    )
    smem = pl.BlockSpec(memory_space=pltpu.SMEM)
    vmem = pl.BlockSpec(memory_space=pltpu.VMEM)
    y_place = lax.axis_index("y").astype(jnp.int32).reshape(1)
    pair_shape = jax.ShapeDtypeStruct(ends.shape, jnp.float32)
    earlier, total = pl.pallas_call(
        combine_body,
        out_shape=(pair_shape, pair_shape),
        in_specs=[smem, vmem],
        out_specs=(vmem, vmem),
        compiler_params=pltpu.CompilerParams(vmem_limit_bytes=8 * 1024 * 1024),
        name="combine",
    )(y_place, sent_to_all(ends, "y"))
    everyone = sent_to_all(total, "z")
    core = lax.axis_index("core")
    place = jnp.stack([lax.axis_index(SP), core, lax.axis_index("z")]).astype(jnp.int32)
    half = length // 2
    width = out_weight.shape[1]
    half_shape = jax.ShapeDtypeStruct((half, width), jnp.bfloat16)
    send, keep = pl.pallas_call(
        carry_body,
        out_shape=(half_shape, half_shape),
        in_specs=[smem] + [vmem] * 5,
        out_specs=(vmem, vmem),
        compiler_params=pltpu.CompilerParams(vmem_limit_bytes=16 * 1024 * 1024),
        name="carry",
    )(place, everyone, earlier, scale, shift, out_weight)

    quarter = half // 2
    even = [(0, 1), (1, 0), (2, 3), (3, 2)]
    odd = [(1, 2), (2, 1), (3, 0), (0, 3)]

    def added(mine, came):
        return (mine.astype(jnp.float32) + came.astype(jnp.float32)).astype(jnp.bfloat16)

    def summed(keep, send):
        came = swap_cores(send)
        low = added(keep[:quarter], came[:quarter])
        high = added(keep[quarter:], came[quarter:])
        low_came = lax.ppermute(low, "x", even)
        high_came = lax.ppermute(high, "x", odd)
        low = added(low, low_came)
        high = added(high, high_came)
        return low, lax.ppermute(low, "x", odd), high, lax.ppermute(high, "x", even)

    middle, near = pl.pallas_call(
        norm_body,
        out_shape=(half_shape, half_shape),
        in_specs=[smem] + [vmem] * 6,
        out_specs=(vmem, vmem),
        compiler_params=pltpu.CompilerParams(vmem_limit_bytes=16 * 1024 * 1024),
        name="norm",
    )(place, residual_in, *summed(keep, send), norm_gain.reshape(1, width))
    far = swap_cores(near)

    parts = 8
    span = width // parts
    send, keep = pl.pallas_call(
        feed_body,
        out_shape=(half_shape, half_shape),
        in_specs=[vmem, vmem, pl.BlockSpec(memory_space=pl.ANY)],
        out_specs=(vmem, vmem),
        scratch_shapes=[
            pltpu.VMEM((length, width), jnp.bfloat16),
            pltpu.VMEM((parts, span, 3 * units), jnp.bfloat16),
            pltpu.VMEM((length, 2 * units), jnp.float32),
            pltpu.VMEM((length, units), jnp.bfloat16),
            pltpu.SemaphoreType.DMA((parts,)),
        ],
        compiler_params=pltpu.CompilerParams(vmem_limit_bytes=28 * 1024 * 1024),
        name="feed",
    )(
        pltpu.with_memory_space_constraint(near, pltpu.VMEM),
        pltpu.with_memory_space_constraint(far, pltpu.VMEM),
        pltpu.with_memory_space_constraint(weights, pltpu.HBM),
    )
    mine = pl.pallas_call(
        finish_body,
        out_shape=half_shape,
        in_specs=[vmem] * 5,
        out_specs=vmem,
        compiler_params=pltpu.CompilerParams(vmem_limit_bytes=8 * 1024 * 1024),
        name="finish",
    )(*(stays(part) for part in (middle, *summed(keep, send))))
    other = swap_cores(mine)

    def written(side, value, *before):
        return pl.pallas_call(
            functools.partial(write_body, side),
            out_shape=jax.ShapeDtypeStruct((length, width), jnp.bfloat16),
            in_specs=[smem, vmem] + [pl.BlockSpec(memory_space=pl.ANY)] * len(before),
            out_specs=pl.BlockSpec(memory_space=pl.ANY),
            scratch_shapes=[pltpu.SemaphoreType.DMA],
            input_output_aliases={2: 0} if before else {},
            compiler_params=pltpu.CompilerParams(vmem_limit_bytes=4 * 1024 * 1024),
            name="write_" + str(side),
        )(place, stays(value), *before)

    return written(1, other, written(0, mine))


def solution(mesh):
    sizes = (8, mesh.shape["sp"] // 8, mesh.shape["tp"] // 2, 2)
    torus = Mesh(mesh.devices.reshape(sizes), ("z", "y", "x", "core"))
    in_specs = (
        P(SP, None),
        P(TP, SP),
        P(TP, SP),
        P(TP, None),
        P(TP, None, None),
        P(TP, None, None),
        P(TP),
        P(TP, SP),
        P(TP, None),
        P(),
        P(SP, TP),
        P(SP, TP),
        P(SP, TP),
    )
    return jax.shard_map(
        on_device, mesh=torus, in_specs=in_specs, out_specs=P(SP, None), check_vma=False
    )
```

```python
import jax
import jax.numpy as jnp
from jax import lax
from jax.experimental import pallas as pl
from jax.experimental.pallas import tpu as pltpu
from jax.sharding import Mesh
from jax.sharding import PartitionSpec as P

SP = ("z", "y")
TP = ("x", "core")


def shifted(value, by, fill):
    rows = value.shape[0]
    head = jnp.full((by, value.shape[1]), fill, value.dtype)
    if by % 8 == 0:
        return jnp.concatenate([head, value[: rows - by]], axis=0)
    rolled = pltpu.roll(value, by, 0)
    row = lax.broadcasted_iota(jnp.int32, value.shape, 0)
    return jnp.where(row < by, jnp.asarray(fill, value.dtype), rolled)


def recurrence_body(
    mixer, before, taps, recur, admit, rate, extra, branch, scale_out, shift_out, ends_out
):
    channels, length = mixer.shape
    tap_count = taps.shape[1]
    signal = mixer[...].astype(jnp.float32).T
    eye = (
        lax.broadcasted_iota(jnp.int32, (channels, channels), 0)
        == lax.broadcasted_iota(jnp.int32, (channels, channels), 1)
    ).astype(jnp.bfloat16)
    turn = (((0,), (0,)), ((), ()))
    tap_rows = lax.dot_general(taps[...], eye, turn, preferred_element_type=jnp.float32)
    halo = lax.dot_general(before[...], eye, turn, preferred_element_type=jnp.float32)
    row = lax.broadcasted_iota(jnp.int32, signal.shape, 0)
    conv_sum = jnp.zeros(signal.shape, jnp.float32)
    for tap in range(tap_count):
        back = tap_count - 1 - tap
        moved = signal
        if back:
            moved = pltpu.roll(signal, back, 0)
            for line in range(back):
                moved = jnp.where(row == line, halo[tap + line : tap + line + 1], moved)
        conv_sum = conv_sum + tap_rows[tap : tap + 1] * moved
    conv_out = conv_sum.astype(jnp.bfloat16)
    groups, width, _ = recur.shape
    spread = (
        lax.broadcasted_iota(jnp.int32, (width, channels), 1) % width
        == lax.broadcasted_iota(jnp.int32, (width, channels), 0)
    ).astype(jnp.bfloat16)
    same = (
        lax.broadcasted_iota(jnp.int32, (channels, channels), 0) // width
        == lax.broadcasted_iota(jnp.int32, (channels, channels), 1) // width
    )

    def gate(weight):
        flat = weight[...].reshape(groups * width, width)
        wide = jnp.dot(flat, spread, preferred_element_type=jnp.float32)
        wide = jnp.where(same, wide, 0.0).astype(jnp.bfloat16)
        return jax.nn.sigmoid(jnp.dot(conv_out, wide, preferred_element_type=jnp.float32))

    recur_gate = gate(recur)
    admit_gate = gate(admit)
    log_decay = -8.0 * recur_gate * rate[...] + extra[...].T
    run = jnp.exp(log_decay)
    twice = 2.0 * log_decay
    series = twice * (1.0 + twice * (0.5 + twice * (1.0 / 6.0 + twice * (1.0 / 24.0 + twice * (
        1.0 / 120.0 + twice * (1.0 / 720.0))))))
    lost = -jnp.where(twice > -0.25, series, run * run - 1.0)
    kept = jnp.where(lost > 0.0, jnp.sqrt(lost), 0.0)
    state = kept * admit_gate * conv_out.astype(jnp.float32)
    by = 1
    while by < length:
        state = state + run * shifted(state, by, 0.0)
        run = run * shifted(run, by, 1.0)
        by *= 2
    ends_out[0:1] = run[length - 1 : length]
    ends_out[1:2] = state[length - 1 : length]
    gelu = jax.nn.gelu(branch[...].astype(jnp.float32), approximate=True).T
    scale_out[...] = run * gelu
    shift_out[...] = state * gelu


def folded(pairs, limit, scale, shift):
    for k in range(pairs.shape[0]):
        pair = pairs[k]
        after_scale, after_shift = pair[0:1] * scale, pair[0:1] * shift + pair[1:2]
        scale = jnp.where(k < limit, after_scale, scale)
        shift = jnp.where(k < limit, after_shift, shift)
    return scale, shift


def combine_body(place, line, before, total):
    one = jnp.ones((1, line.shape[2]), jnp.float32)
    for target, limit in ((before, place[0]), (total, line.shape[0])):
        scale, shift = folded(line, limit, one, 0.0 * one)
        target[0:1] = scale
        target[1:2] = shift


def carry_body(place, rows, before, scale, shift, weight, send, keep):
    core, z = place[1], place[2]
    half = send.shape[0]
    one = jnp.ones((1, scale.shape[1]), jnp.float32)
    entering = folded(rows, z, one, 0.0 * one)[1]
    entering = before[0:1] * entering + before[1:2]
    for target, side in ((send, 1 - core), (keep, core)):
        at = pl.ds(pl.multiple_of(side * half, half), half)
        mixed = (shift[at, :] + scale[at, :] * entering).astype(jnp.bfloat16)
        found = jnp.dot(mixed, weight[...], preferred_element_type=jnp.float32)
        target[...] = found.astype(jnp.bfloat16)


def norm_body(place, residual, low, low_came, high, high_came, gain, middle, normed):
    half = middle.shape[0]
    quarter = half // 2
    for at, mine, came in ((0, low, low_came), (quarter, high, high_came)):
        branch = mine[...].astype(jnp.float32) + came[...].astype(jnp.float32)
        rows = pl.ds(pl.multiple_of(place[1] * half + at, quarter), quarter)
        found = (residual[rows, :].astype(jnp.float32) + branch).astype(jnp.bfloat16)
        middle[at : at + quarter, :] = found
        wide = found.astype(jnp.float32)
        row_scale = lax.rsqrt(jnp.mean(wide * wide, axis=1, keepdims=True) + 1e-06)
        ready = wide * row_scale * gain[...].astype(jnp.float32)
        normed[at : at + quarter, :] = ready.astype(jnp.bfloat16)


def finish_body(middle, low, low_came, high, high_came, out):
    quarter = low.shape[0]
    for at, mine, came in ((0, low, low_came), (quarter, high, high_came)):
        rows = pl.ds(at, quarter)
        channel_out = mine[...].astype(jnp.float32) + came[...].astype(jnp.float32)
        out[rows, :] = (middle[rows, :].astype(jnp.float32) + channel_out).astype(jnp.bfloat16)


def feed_body(near, far, weights, send, keep, rows, stage, both_sum, hidden, arrived):
    parts, span, _ = stage.shape
    half = near.shape[0]
    units = hidden.shape[1]
    copies = [
        pltpu.make_async_copy(weights.at[pl.ds(k * span, span), :], stage.at[k], arrived.at[k])
        for k in range(parts)
    ]
    for copy in copies:
        copy.start()
    rows[:half] = near[...]
    rows[half:] = far[...]
    for k in range(0, parts, 2):
        found = None
        for piece in (k, k + 1):
            copies[piece].wait()
            part = jnp.dot(
                rows[:, piece * span : (piece + 1) * span],
                stage[piece, :, : 2 * units],
                preferred_element_type=jnp.float32,
            )
            found = part if found is None else found + part
        if k == 0:
            both_sum[...] = found
        else:
            both_sum[...] += found
    gated = both_sum[:, :units]
    silu = gated / (1.0 + jnp.exp(-gated))
    hidden[...] = (silu * both_sum[:, units:]).astype(jnp.bfloat16)
    flip = (((1,), (1,)), ((), ()))
    for k in range(parts):
        down = stage[k, :, 2 * units :]
        found = lax.dot_general(hidden[...], down, flip, preferred_element_type=jnp.float32)
        keep[:, k * span : (k + 1) * span] = found[:half].astype(jnp.bfloat16)
        send[:, k * span : (k + 1) * span] = found[half:].astype(jnp.bfloat16)


def sent_to_all(value, axis):
    count = lax.axis_size(axis)
    return lax.all_to_all(
        jnp.broadcast_to(value[None], (count, *value.shape)), axis, 0, 0, tiled=True
    )


def stays(value):
    return pltpu.with_memory_space_constraint(value, pltpu.VMEM)


def swap_cores(value):
    return lax.ppermute(value, "core", [(0, 1), (1, 0)])


def on_device(
    residual_in,
    mixer_input,
    branch_gate,
    conv_taps,
    recur_weight,
    admit_weight,
    decay_param,
    decay_extra,
    out_weight,
    norm_gain,
    gate_weight,
    up_weight,
    down_weight,
):
    units = gate_weight.shape[1]
    weights = jnp.concatenate([gate_weight, up_weight, down_weight], axis=1)
    weights = lax.all_gather(weights, SP, axis=0, tiled=True)

    channels, length = mixer_input.shape
    tap_count = conv_taps.shape[1]
    count = lax.axis_size(SP)
    tail = mixer_input[:, length - (tap_count - 1) :]
    before = lax.ppermute(tail, SP, [(i, i + 1) for i in range(count - 1)])
    square = jax.ShapeDtypeStruct((length, channels), jnp.float32)
    scale, shift, ends = pl.pallas_call(
        recurrence_body,
        out_shape=(square, square, jax.ShapeDtypeStruct((2, channels), jnp.float32)),
        in_specs=[pl.BlockSpec(memory_space=pltpu.VMEM)] * 8,
        out_specs=(pl.BlockSpec(memory_space=pltpu.VMEM),) * 3,
        compiler_params=pltpu.CompilerParams(vmem_limit_bytes=16 * 1024 * 1024),
        name="recurrence",
    )(
        mixer_input,
        before,
        conv_taps,
        recur_weight,
        admit_weight,
        jax.nn.softplus(-decay_param).reshape(1, channels),
        decay_extra,
        branch_gate,
    )
    smem = pl.BlockSpec(memory_space=pltpu.SMEM)
    vmem = pl.BlockSpec(memory_space=pltpu.VMEM)
    y_place = lax.axis_index("y").astype(jnp.int32).reshape(1)
    pair_shape = jax.ShapeDtypeStruct(ends.shape, jnp.float32)
    earlier, total = pl.pallas_call(
        combine_body,
        out_shape=(pair_shape, pair_shape),
        in_specs=[smem, vmem],
        out_specs=(vmem, vmem),
        compiler_params=pltpu.CompilerParams(vmem_limit_bytes=8 * 1024 * 1024),
        name="combine",
    )(y_place, sent_to_all(ends, "y"))
    everyone = sent_to_all(total, "z")
    core = lax.axis_index("core")
    place = jnp.stack([lax.axis_index(SP), core, lax.axis_index("z")]).astype(jnp.int32)
    half = length // 2
    width = out_weight.shape[1]
    half_shape = jax.ShapeDtypeStruct((half, width), jnp.bfloat16)
    send, keep = pl.pallas_call(
        carry_body,
        out_shape=(half_shape, half_shape),
        in_specs=[smem] + [vmem] * 5,
        out_specs=(vmem, vmem),
        compiler_params=pltpu.CompilerParams(vmem_limit_bytes=16 * 1024 * 1024),
        name="carry",
    )(place, everyone, earlier, scale, shift, out_weight)

    quarter = half // 2
    even = [(0, 1), (1, 0), (2, 3), (3, 2)]
    odd = [(1, 2), (2, 1), (3, 0), (0, 3)]

    def added(mine, came):
        return (mine.astype(jnp.float32) + came.astype(jnp.float32)).astype(jnp.bfloat16)

    def summed(keep, send):
        came = swap_cores(send)
        low = added(keep[:quarter], came[:quarter])
        high = added(keep[quarter:], came[quarter:])
        low_came = lax.ppermute(low, "x", odd)
        high_came = lax.ppermute(high, "x", even)
        low = added(low, low_came)
        high = added(high, high_came)
        return low, lax.ppermute(low, "x", even), high, lax.ppermute(high, "x", odd)

    middle, near = pl.pallas_call(
        norm_body,
        out_shape=(half_shape, half_shape),
        in_specs=[smem] + [vmem] * 6,
        out_specs=(vmem, vmem),
        compiler_params=pltpu.CompilerParams(vmem_limit_bytes=16 * 1024 * 1024),
        name="norm",
    )(place, residual_in, *summed(keep, send), norm_gain.reshape(1, width))
    far = swap_cores(near)

    parts = 8
    span = width // parts
    send, keep = pl.pallas_call(
        feed_body,
        out_shape=(half_shape, half_shape),
        in_specs=[vmem, vmem, pl.BlockSpec(memory_space=pl.ANY)],
        out_specs=(vmem, vmem),
        scratch_shapes=[
            pltpu.VMEM((length, width), jnp.bfloat16),
            pltpu.VMEM((parts, span, 3 * units), jnp.bfloat16),
            pltpu.VMEM((length, 2 * units), jnp.float32),
            pltpu.VMEM((length, units), jnp.bfloat16),
            pltpu.SemaphoreType.DMA((parts,)),
        ],
        compiler_params=pltpu.CompilerParams(vmem_limit_bytes=28 * 1024 * 1024),
        name="feed",
    )(
        pltpu.with_memory_space_constraint(near, pltpu.VMEM),
        pltpu.with_memory_space_constraint(far, pltpu.VMEM),
        pltpu.with_memory_space_constraint(weights, pltpu.HBM),
    )
    mine = pl.pallas_call(
        finish_body,
        out_shape=half_shape,
        in_specs=[vmem] * 5,
        out_specs=vmem,
        compiler_params=pltpu.CompilerParams(vmem_limit_bytes=8 * 1024 * 1024),
        name="finish",
    )(*(stays(part) for part in (middle, *summed(keep, send))))
    other = swap_cores(mine)

    first = jnp.where(core == 0, mine, other)
    last = jnp.where(core == 0, other, mine)
    return jnp.concatenate([first, last], axis=0)


def solution(mesh):
    sizes = (8, mesh.shape["sp"] // 8, mesh.shape["tp"] // 2, 2)
    torus = Mesh(mesh.devices.reshape(sizes), ("z", "y", "x", "core"))
    in_specs = (
        P(SP, None),
        P(TP, SP),
        P(TP, SP),
        P(TP, None),
        P(TP, None, None),
        P(TP, None, None),
        P(TP),
        P(TP, SP),
        P(TP, None),
        P(),
        P(SP, TP),
        P(SP, TP),
        P(SP, TP),
    )
    return jax.shard_map(
        on_device, mesh=torus, in_specs=in_specs, out_specs=P(SP, None), check_vma=False
    )
```

```python
import jax
import jax.numpy as jnp
from jax import lax
from jax.experimental import pallas as pl
from jax.experimental.pallas import tpu as pltpu
from jax.sharding import Mesh
from jax.sharding import PartitionSpec as P

SP = ("z", "y")
TP = ("x", "core")


def shifted(value, by, fill):
    rows = value.shape[0]
    head = jnp.full((by, value.shape[1]), fill, value.dtype)
    if by % 8 == 0:
        return jnp.concatenate([head, value[: rows - by]], axis=0)
    rolled = pltpu.roll(value, by, 0)
    row = lax.broadcasted_iota(jnp.int32, value.shape, 0)
    return jnp.where(row < by, jnp.asarray(fill, value.dtype), rolled)


def recurrence_body(
    mixer, before, taps, recur, admit, rate, extra, branch, scale_out, shift_out, ends_out
):
    channels, length = mixer.shape
    tap_count = taps.shape[1]
    signal = mixer[...].astype(jnp.float32).T
    eye = (
        lax.broadcasted_iota(jnp.int32, (channels, channels), 0)
        == lax.broadcasted_iota(jnp.int32, (channels, channels), 1)
    ).astype(jnp.bfloat16)
    turn = (((0,), (0,)), ((), ()))
    tap_rows = lax.dot_general(taps[...], eye, turn, preferred_element_type=jnp.float32)
    halo = lax.dot_general(before[...], eye, turn, preferred_element_type=jnp.float32)
    row = lax.broadcasted_iota(jnp.int32, signal.shape, 0)
    conv_sum = jnp.zeros(signal.shape, jnp.float32)
    for tap in range(tap_count):
        back = tap_count - 1 - tap
        moved = signal
        if back:
            moved = pltpu.roll(signal, back, 0)
            for line in range(back):
                moved = jnp.where(row == line, halo[tap + line : tap + line + 1], moved)
        conv_sum = conv_sum + tap_rows[tap : tap + 1] * moved
    conv_out = conv_sum.astype(jnp.bfloat16)
    groups, width, _ = recur.shape
    spread = (
        lax.broadcasted_iota(jnp.int32, (width, channels), 1) % width
        == lax.broadcasted_iota(jnp.int32, (width, channels), 0)
    ).astype(jnp.bfloat16)
    same = (
        lax.broadcasted_iota(jnp.int32, (channels, channels), 0) // width
        == lax.broadcasted_iota(jnp.int32, (channels, channels), 1) // width
    )

    def gate(weight):
        flat = weight[...].reshape(groups * width, width)
        wide = jnp.dot(flat, spread, preferred_element_type=jnp.float32)
        wide = jnp.where(same, wide, 0.0).astype(jnp.bfloat16)
        return jax.nn.sigmoid(jnp.dot(conv_out, wide, preferred_element_type=jnp.float32))

    recur_gate = gate(recur)
    admit_gate = gate(admit)
    log_decay = -8.0 * recur_gate * rate[...] + extra[...].T
    run = jnp.exp(log_decay)
    twice = 2.0 * log_decay
    series = twice * (1.0 + twice * (0.5 + twice * (1.0 / 6.0 + twice * (1.0 / 24.0 + twice * (
        1.0 / 120.0 + twice * (1.0 / 720.0))))))
    lost = -jnp.where(twice > -0.25, series, run * run - 1.0)
    kept = jnp.where(lost > 0.0, jnp.sqrt(lost), 0.0)
    state = kept * admit_gate * conv_out.astype(jnp.float32)
    by = 1
    while by < length:
        state = state + run * shifted(state, by, 0.0)
        run = run * shifted(run, by, 1.0)
        by *= 2
    ends_out[0:1] = run[length - 1 : length]
    ends_out[1:2] = state[length - 1 : length]
    gelu = jax.nn.gelu(branch[...].astype(jnp.float32), approximate=True).T
    scale_out[...] = run * gelu
    shift_out[...] = state * gelu


def folded(pairs, limit, scale, shift):
    for k in range(pairs.shape[0]):
        pair = pairs[k]
        after_scale, after_shift = pair[0:1] * scale, pair[0:1] * shift + pair[1:2]
        scale = jnp.where(k < limit, after_scale, scale)
        shift = jnp.where(k < limit, after_shift, shift)
    return scale, shift


def combine_body(place, line, before, total):
    one = jnp.ones((1, line.shape[2]), jnp.float32)
    for target, limit in ((before, place[0]), (total, line.shape[0])):
        scale, shift = folded(line, limit, one, 0.0 * one)
        target[0:1] = scale
        target[1:2] = shift


def carry_body(place, rows, before, scale, shift, weight, send, keep):
    core, z = place[1], place[2]
    half = send.shape[0]
    one = jnp.ones((1, scale.shape[1]), jnp.float32)
    entering = folded(rows, z, one, 0.0 * one)[1]
    entering = before[0:1] * entering + before[1:2]
    for target, side in ((send, 1 - core), (keep, core)):
        at = pl.ds(pl.multiple_of(side * half, half), half)
        mixed = (shift[at, :] + scale[at, :] * entering).astype(jnp.bfloat16)
        found = jnp.dot(mixed, weight[...], preferred_element_type=jnp.float32)
        target[...] = found.astype(jnp.bfloat16)


def norm_body(place, residual, mine, came, gain, middle, normed):
    half = middle.shape[0]
    branch = mine[...].astype(jnp.float32) + came[...].astype(jnp.float32)
    rows = pl.ds(pl.multiple_of(place[1] * half, half), half)
    found = (residual[rows, :].astype(jnp.float32) + branch).astype(jnp.bfloat16)
    middle[...] = found
    wide = found.astype(jnp.float32)
    row_scale = lax.rsqrt(jnp.mean(wide * wide, axis=1, keepdims=True) + 1e-06)
    normed[...] = (wide * row_scale * gain[...].astype(jnp.float32)).astype(jnp.bfloat16)


def pack_body(gate, up, down, out):
    rows, units = gate.shape
    wide = out.shape[1]
    blocks = 3 * units // wide
    spare = 3 * units - blocks * wide
    last = down[...].astype(jnp.float32)[:, units - spare :]
    parts = [gate[...].astype(jnp.float32), up[...].astype(jnp.float32)]
    parts.append(down[...].astype(jnp.float32)[:, : units - spare])
    joined = jnp.concatenate(parts, axis=1)
    for k in range(blocks):
        piece = joined[:, k * wide : (k + 1) * wide].astype(out.dtype)
        out[k * rows : (k + 1) * rows, :] = piece
    lines = rows * spare // wide
    lot = [last[k * lines : (k + 1) * lines] for k in range(rows // lines)]
    out[blocks * rows :, :] = jnp.concatenate(lot, axis=1).astype(out.dtype)


def feed_body(near, far, weights, send, keep, rows, stage, rest, both_sum, hidden, arrived):
    blocks, shards, share, wide = stage.shape
    half = near.shape[0]
    units = hidden.shape[1]
    lines = rest.shape[1]
    spare = rest.shape[1] * wide // share
    copies = [
        pltpu.make_async_copy(
            weights.at[:, pl.ds(k * share, share), :], stage.at[k], arrived.at[k]
        )
        for k in range(blocks)
    ]
    copies.append(
        pltpu.make_async_copy(
            weights.at[:, pl.ds(blocks * share, lines), :], rest, arrived.at[blocks]
        )
    )
    for copy in copies:
        copy.start()
    rows[:half] = near[...]
    rows[half:] = far[...]
    both = 2 * units
    for k in range(-(-both // wide)):
        copies[k].wait()
        columns = min(wide, both - k * wide)
        weight = stage[k].reshape(shards * share, wide)[:, :columns]
        found = jnp.dot(rows[...], weight, preferred_element_type=jnp.float32)
        both_sum[:, k * wide : k * wide + columns] = found
    gated = both_sum[:, :units]
    silu = gated / (1.0 + jnp.exp(-gated))
    hidden[...] = (silu * both_sum[:, units:]).astype(jnp.bfloat16)
    for k in range(-(-both // wide), blocks + 1):
        copies[k].wait()
    loose = rest[...].astype(jnp.float32)
    loose = jnp.concatenate(
        [loose[:, :, k * spare : (k + 1) * spare] for k in range(wide // spare)], axis=1
    ).astype(jnp.bfloat16)
    first = both // wide
    step = 256 // share
    flip = (((1,), (1,)), ((), ()))
    for at in range(0, shards, step):
        found, used = None, 0
        for k in range(first, blocks + 1):
            if k < blocks:
                start = both - first * wide if k == first else 0
                weight = stage[k, at : at + step].reshape(step * share, wide)[:, start:]
            else:
                weight = loose[at : at + step].reshape(step * share, spare)
            count = weight.shape[1]
            piece = hidden[:, used : used + count]
            part = lax.dot_general(piece, weight, flip, preferred_element_type=jnp.float32)
            found = part if found is None else found + part
            used += count
        columns = slice(at * share, (at + step) * share)
        keep[:, columns] = found[:half].astype(jnp.bfloat16)
        send[:, columns] = found[half:].astype(jnp.bfloat16)


def sent_to_all(value, axis):
    count = lax.axis_size(axis)
    return lax.all_to_all(
        jnp.broadcast_to(value[None], (count, *value.shape)), axis, 0, 0, tiled=True
    )


def swap_cores(value):
    return lax.ppermute(value, "core", [(0, 1), (1, 0)])


def on_device(
    residual_in,
    mixer_input,
    branch_gate,
    conv_taps,
    recur_weight,
    admit_weight,
    decay_param,
    decay_extra,
    out_weight,
    norm_gain,
    gate_weight,
    up_weight,
    down_weight,
):
    shard, units = gate_weight.shape
    wide = 256
    lot = 3 * units * shard // wide
    weights = pl.pallas_call(
        pack_body,
        out_shape=jax.ShapeDtypeStruct((lot, wide), gate_weight.dtype),
        compiler_params=pltpu.CompilerParams(vmem_limit_bytes=8 * 1024 * 1024),
        name="pack",
    )(*(pltpu.with_memory_space_constraint(w, pltpu.HBM) for w in (gate_weight, up_weight, down_weight)))
    weights = lax.all_gather(weights, SP, axis=0)

    channels, length = mixer_input.shape
    tap_count = conv_taps.shape[1]
    count = lax.axis_size(SP)
    tail = mixer_input[:, length - (tap_count - 1) :]
    before = lax.ppermute(tail, SP, [(i, i + 1) for i in range(count - 1)])
    square = jax.ShapeDtypeStruct((length, channels), jnp.float32)
    scale, shift, ends = pl.pallas_call(
        recurrence_body,
        out_shape=(square, square, jax.ShapeDtypeStruct((2, channels), jnp.float32)),
        in_specs=[pl.BlockSpec(memory_space=pltpu.VMEM)] * 8,
        out_specs=(pl.BlockSpec(memory_space=pltpu.VMEM),) * 3,
        compiler_params=pltpu.CompilerParams(vmem_limit_bytes=16 * 1024 * 1024),
        name="recurrence",
    )(
        mixer_input,
        before,
        conv_taps,
        recur_weight,
        admit_weight,
        jax.nn.softplus(-decay_param).reshape(1, channels),
        decay_extra,
        branch_gate,
    )
    smem = pl.BlockSpec(memory_space=pltpu.SMEM)
    vmem = pl.BlockSpec(memory_space=pltpu.VMEM)
    y_place = lax.axis_index("y").astype(jnp.int32).reshape(1)
    pair_shape = jax.ShapeDtypeStruct(ends.shape, jnp.float32)
    earlier, total = pl.pallas_call(
        combine_body,
        out_shape=(pair_shape, pair_shape),
        in_specs=[smem, vmem],
        out_specs=(vmem, vmem),
        compiler_params=pltpu.CompilerParams(vmem_limit_bytes=8 * 1024 * 1024),
        name="combine",
    )(y_place, sent_to_all(ends, "y"))
    everyone = sent_to_all(total, "z")
    core = lax.axis_index("core")
    place = jnp.stack([lax.axis_index(SP), core, lax.axis_index("z")]).astype(jnp.int32)
    half = length // 2
    width = out_weight.shape[1]
    half_shape = jax.ShapeDtypeStruct((half, width), jnp.bfloat16)
    send, keep = pl.pallas_call(
        carry_body,
        out_shape=(half_shape, half_shape),
        in_specs=[smem] + [vmem] * 5,
        out_specs=(vmem, vmem),
        compiler_params=pltpu.CompilerParams(vmem_limit_bytes=16 * 1024 * 1024),
        name="carry",
    )(place, everyone, earlier, scale, shift, out_weight)

    even, odd = (1, 0, 3, 2), (3, 2, 1, 0)

    def added(mine, came):
        return (mine.astype(jnp.float32) + came.astype(jnp.float32)).astype(jnp.bfloat16)

    def paired(value, by_core):
        pairs = [(2 * x + c, 2 * by_core[c][x] + c) for x in range(4) for c in range(2)]
        return lax.ppermute(value, TP, pairs)

    def summed(keep, send):
        mine = added(keep, swap_cores(send))
        mine = added(mine, paired(mine, (even, odd)))
        return mine, paired(mine, (odd, even))

    middle, near = pl.pallas_call(
        norm_body,
        out_shape=(half_shape, half_shape),
        in_specs=[smem] + [vmem] * 4,
        out_specs=(vmem, vmem),
        compiler_params=pltpu.CompilerParams(vmem_limit_bytes=16 * 1024 * 1024),
        name="norm",
    )(place, residual_in, *summed(keep, send), norm_gain.reshape(1, width))
    far = swap_cores(near)

    blocks = 3 * units // wide
    lines = lot - blocks * shard
    send, keep = pl.pallas_call(
        feed_body,
        out_shape=(half_shape, half_shape),
        in_specs=[vmem, vmem, pl.BlockSpec(memory_space=pl.ANY)],
        out_specs=(vmem, vmem),
        scratch_shapes=[
            pltpu.VMEM((length, width), jnp.bfloat16),
            pltpu.VMEM((blocks, count, shard, wide), jnp.bfloat16),
            pltpu.VMEM((count, lines, wide), jnp.bfloat16),
            pltpu.VMEM((length, 2 * units), jnp.float32),
            pltpu.VMEM((length, units), jnp.bfloat16),
            pltpu.SemaphoreType.DMA((blocks + 1,)),
        ],
        compiler_params=pltpu.CompilerParams(vmem_limit_bytes=28 * 1024 * 1024),
        name="feed",
    )(
        pltpu.with_memory_space_constraint(near, pltpu.VMEM),
        pltpu.with_memory_space_constraint(far, pltpu.VMEM),
        pltpu.with_memory_space_constraint(weights, pltpu.HBM),
    )
    mine, came = summed(keep, send)
    channel_out = mine.astype(jnp.float32) + came.astype(jnp.float32)
    mine = (middle.astype(jnp.float32) + channel_out).astype(jnp.bfloat16)
    other = swap_cores(mine)
    first = jnp.where(core == 0, mine, other)
    last = jnp.where(core == 0, other, mine)
    return jnp.concatenate([first, last], axis=0)


def solution(mesh):
    sizes = (8, mesh.shape["sp"] // 8, mesh.shape["tp"] // 2, 2)
    torus = Mesh(mesh.devices.reshape(sizes), ("z", "y", "x", "core"))
    in_specs = (
        P(SP, None),
        P(TP, SP),
        P(TP, SP),
        P(TP, None),
        P(TP, None, None),
        P(TP, None, None),
        P(TP),
        P(TP, SP),
        P(TP, None),
        P(),
        P(SP, TP),
        P(SP, TP),
        P(SP, TP),
    )
    return jax.shard_map(
        on_device, mesh=torus, in_specs=in_specs, out_specs=P(SP, None), check_vma=False
    )
```

```python
import jax
import jax.numpy as jnp
from jax import lax
from jax.experimental import pallas as pl
from jax.experimental.pallas import tpu as pltpu
from jax.sharding import Mesh
from jax.sharding import PartitionSpec as P

SP = ("z", "y")
TP = ("x", "core")


def shifted(value, by, fill):
    rows = value.shape[0]
    head = jnp.full((by, value.shape[1]), fill, value.dtype)
    if by % 8 == 0:
        return jnp.concatenate([head, value[: rows - by]], axis=0)
    rolled = pltpu.roll(value, by, 0)
    row = lax.broadcasted_iota(jnp.int32, value.shape, 0)
    return jnp.where(row < by, jnp.asarray(fill, value.dtype), rolled)


def recurrence_body(
    mixer, before, taps, recur, admit, rate, extra, branch, scale_out, shift_out, ends_out
):
    channels, length = mixer.shape
    tap_count = taps.shape[1]
    signal = mixer[...].astype(jnp.float32).T
    eye = (
        lax.broadcasted_iota(jnp.int32, (channels, channels), 0)
        == lax.broadcasted_iota(jnp.int32, (channels, channels), 1)
    ).astype(jnp.bfloat16)
    turn = (((0,), (0,)), ((), ()))
    tap_rows = lax.dot_general(taps[...], eye, turn, preferred_element_type=jnp.float32)
    halo = lax.dot_general(before[...], eye, turn, preferred_element_type=jnp.float32)
    row = lax.broadcasted_iota(jnp.int32, signal.shape, 0)
    conv_sum = jnp.zeros(signal.shape, jnp.float32)
    for tap in range(tap_count):
        back = tap_count - 1 - tap
        moved = signal
        if back:
            moved = pltpu.roll(signal, back, 0)
            for line in range(back):
                moved = jnp.where(row == line, halo[tap + line : tap + line + 1], moved)
        conv_sum = conv_sum + tap_rows[tap : tap + 1] * moved
    conv_out = conv_sum.astype(jnp.bfloat16)
    groups, width, _ = recur.shape
    spread = (
        lax.broadcasted_iota(jnp.int32, (width, channels), 1) % width
        == lax.broadcasted_iota(jnp.int32, (width, channels), 0)
    ).astype(jnp.bfloat16)
    same = (
        lax.broadcasted_iota(jnp.int32, (channels, channels), 0) // width
        == lax.broadcasted_iota(jnp.int32, (channels, channels), 1) // width
    )

    def gate(weight):
        flat = weight[...].reshape(groups * width, width)
        wide = jnp.dot(flat, spread, preferred_element_type=jnp.float32)
        wide = jnp.where(same, wide, 0.0).astype(jnp.bfloat16)
        return jax.nn.sigmoid(jnp.dot(conv_out, wide, preferred_element_type=jnp.float32))

    recur_gate = gate(recur)
    admit_gate = gate(admit)
    log_decay = -8.0 * recur_gate * rate[...] + extra[...].T
    run = jnp.exp(log_decay)
    twice = 2.0 * log_decay
    series = twice * (1.0 + twice * (0.5 + twice * (1.0 / 6.0 + twice * (1.0 / 24.0 + twice * (
        1.0 / 120.0 + twice * (1.0 / 720.0))))))
    lost = -jnp.where(twice > -0.25, series, run * run - 1.0)
    kept = jnp.where(lost > 0.0, jnp.sqrt(lost), 0.0)
    state = kept * admit_gate * conv_out.astype(jnp.float32)
    by = 1
    while by < length:
        state = state + run * shifted(state, by, 0.0)
        run = run * shifted(run, by, 1.0)
        by *= 2
    ends_out[0:1] = run[length - 1 : length]
    ends_out[1:2] = state[length - 1 : length]
    gelu = jax.nn.gelu(branch[...].astype(jnp.float32), approximate=True).T
    scale_out[...] = run * gelu
    shift_out[...] = state * gelu


def folded(pairs, limit, scale, shift):
    for k in range(pairs.shape[0]):
        pair = pairs[k]
        after_scale, after_shift = pair[0:1] * scale, pair[0:1] * shift + pair[1:2]
        scale = jnp.where(k < limit, after_scale, scale)
        shift = jnp.where(k < limit, after_shift, shift)
    return scale, shift


def combine_body(place, line, before, total):
    one = jnp.ones((1, line.shape[2]), jnp.float32)
    for target, limit in ((before, place[0]), (total, line.shape[0])):
        scale, shift = folded(line, limit, one, 0.0 * one)
        target[0:1] = scale
        target[1:2] = shift


def carry_body(place, rows, before, scale, shift, weight, send, keep):
    core, z = place[1], place[2]
    half = send.shape[0]
    one = jnp.ones((1, scale.shape[1]), jnp.float32)
    entering = folded(rows, z, one, 0.0 * one)[1]
    entering = before[0:1] * entering + before[1:2]
    for target, side in ((send, 1 - core), (keep, core)):
        at = pl.ds(pl.multiple_of(side * half, half), half)
        mixed = (shift[at, :] + scale[at, :] * entering).astype(jnp.bfloat16)
        found = jnp.dot(mixed, weight[...], preferred_element_type=jnp.float32)
        target[...] = found.astype(jnp.bfloat16)


def norm_body(place, residual, mine, came, gain, middle, normed):
    half = middle.shape[0]
    branch = mine[...].astype(jnp.float32) + came[...].astype(jnp.float32)
    rows = pl.ds(pl.multiple_of(place[1] * half, half), half)
    found = (residual[rows, :].astype(jnp.float32) + branch).astype(jnp.bfloat16)
    middle[...] = found
    wide = found.astype(jnp.float32)
    row_scale = lax.rsqrt(jnp.mean(wide * wide, axis=1, keepdims=True) + 1e-06)
    normed[...] = (wide * row_scale * gain[...].astype(jnp.float32)).astype(jnp.bfloat16)


def pack_body(gate, up, down, out):
    rows, units = gate.shape
    wide = out.shape[1]
    blocks = 3 * units // wide
    spare = 3 * units - blocks * wide
    last = down[...].astype(jnp.float32)[:, units - spare :]
    parts = [down[...].astype(jnp.float32)[:, : units - spare]]
    parts += [gate[...].astype(jnp.float32), up[...].astype(jnp.float32)]
    joined = jnp.concatenate(parts, axis=1)
    for k in range(blocks):
        piece = joined[:, k * wide : (k + 1) * wide].astype(out.dtype)
        out[k * rows : (k + 1) * rows, :] = piece
    lines = rows * spare // wide
    lot = [last[k * lines : (k + 1) * lines] for k in range(rows // lines)]
    out[blocks * rows :, :] = jnp.concatenate(lot, axis=1).astype(out.dtype)


def feed_body(near, far, weights, send, keep, rows, stage, tail, both_sum, hidden, arrived):
    parts, group, lot, wide = stage.shape
    half = near.shape[0]
    units = hidden.shape[1]
    blocks = 3 * units // wide
    share = rows.shape[1] // (parts * group)
    span = group * share
    spare = 3 * units - blocks * wide
    full = (units - spare) // wide
    begin = units - spare - full * wide
    copies = [
        pltpu.make_async_copy(weights.at[pl.ds(k * group, group)], stage.at[k], arrived.at[k])
        for k in range(parts)
    ]
    for copy in copies:
        copy.start()
    rows[:half] = near[...]
    rows[half:] = far[...]

    def block(k, at):
        return stage[k, :, at * share : (at + 1) * share, :].reshape(span, wide)

    for k in range(0, parts, 2):
        for piece in (k, k + 1):
            copies[piece].wait()
            loose = stage[piece, :, blocks * share :, :].astype(jnp.float32)
            loose = [loose[:, :, at * spare : (at + 1) * spare] for at in range(wide // spare)]
            loose = jnp.concatenate(loose, axis=1).astype(tail.dtype).reshape(span, spare)
            tail[piece, :, :begin] = block(piece, full)[:, :begin]
            tail[piece, :, begin:] = loose
        for at in range(full, blocks):
            start = begin if at == full else 0
            found = None
            for piece in (k, k + 1):
                weight = block(piece, at)[:, start:]
                mine = rows[:, piece * span : (piece + 1) * span]
                part = jnp.dot(mine, weight, preferred_element_type=jnp.float32)
                found = part if found is None else found + part
            first = at * wide + start - (units - spare)
            columns = slice(first, first + wide - start)
            if k == 0:
                both_sum[:, columns] = found
            else:
                both_sum[:, columns] += found
    gated = both_sum[:, :units]
    silu = gated / (1.0 + jnp.exp(-gated))
    hidden[...] = (silu * both_sum[:, units:]).astype(jnp.bfloat16)
    flip = (((1,), (1,)), ((), ()))
    for k in range(parts):
        found = lax.dot_general(
            hidden[:, full * wide :], tail[k], flip, preferred_element_type=jnp.float32
        )
        for at in range(full):
            piece = hidden[:, at * wide : (at + 1) * wide]
            found = found + lax.dot_general(
                piece, block(k, at), flip, preferred_element_type=jnp.float32
            )
        keep[:, k * span : (k + 1) * span] = found[:half].astype(jnp.bfloat16)
        send[:, k * span : (k + 1) * span] = found[half:].astype(jnp.bfloat16)


def sent_to_all(value, axis):
    count = lax.axis_size(axis)
    return lax.all_to_all(
        jnp.broadcast_to(value[None], (count, *value.shape)), axis, 0, 0, tiled=True
    )


def swap_cores(value):
    return lax.ppermute(value, "core", [(0, 1), (1, 0)])


def on_device(
    residual_in,
    mixer_input,
    branch_gate,
    conv_taps,
    recur_weight,
    admit_weight,
    decay_param,
    decay_extra,
    out_weight,
    norm_gain,
    gate_weight,
    up_weight,
    down_weight,
):
    shard, units = gate_weight.shape
    wide = 256
    lot = 3 * units * shard // wide
    weights = pl.pallas_call(
        pack_body,
        out_shape=jax.ShapeDtypeStruct((lot, wide), gate_weight.dtype),
        compiler_params=pltpu.CompilerParams(vmem_limit_bytes=8 * 1024 * 1024),
        name="pack",
    )(*(pltpu.with_memory_space_constraint(w, pltpu.HBM) for w in (gate_weight, up_weight, down_weight)))
    weights = lax.all_gather(weights, SP, axis=0)

    channels, length = mixer_input.shape
    tap_count = conv_taps.shape[1]
    count = lax.axis_size(SP)
    tail = mixer_input[:, length - (tap_count - 1) :]
    before = lax.ppermute(tail, SP, [(i, i + 1) for i in range(count - 1)])
    square = jax.ShapeDtypeStruct((length, channels), jnp.float32)
    scale, shift, ends = pl.pallas_call(
        recurrence_body,
        out_shape=(square, square, jax.ShapeDtypeStruct((2, channels), jnp.float32)),
        in_specs=[pl.BlockSpec(memory_space=pltpu.VMEM)] * 8,
        out_specs=(pl.BlockSpec(memory_space=pltpu.VMEM),) * 3,
        compiler_params=pltpu.CompilerParams(vmem_limit_bytes=16 * 1024 * 1024),
        name="recurrence",
    )(
        mixer_input,
        before,
        conv_taps,
        recur_weight,
        admit_weight,
        jax.nn.softplus(-decay_param).reshape(1, channels),
        decay_extra,
        branch_gate,
    )
    smem = pl.BlockSpec(memory_space=pltpu.SMEM)
    vmem = pl.BlockSpec(memory_space=pltpu.VMEM)
    y_place = lax.axis_index("y").astype(jnp.int32).reshape(1)
    pair_shape = jax.ShapeDtypeStruct(ends.shape, jnp.float32)
    earlier, total = pl.pallas_call(
        combine_body,
        out_shape=(pair_shape, pair_shape),
        in_specs=[smem, vmem],
        out_specs=(vmem, vmem),
        compiler_params=pltpu.CompilerParams(vmem_limit_bytes=8 * 1024 * 1024),
        name="combine",
    )(y_place, sent_to_all(ends, "y"))
    everyone = sent_to_all(total, "z")
    core = lax.axis_index("core")
    place = jnp.stack([lax.axis_index(SP), core, lax.axis_index("z")]).astype(jnp.int32)
    half = length // 2
    width = out_weight.shape[1]
    half_shape = jax.ShapeDtypeStruct((half, width), jnp.bfloat16)
    send, keep = pl.pallas_call(
        carry_body,
        out_shape=(half_shape, half_shape),
        in_specs=[smem] + [vmem] * 5,
        out_specs=(vmem, vmem),
        compiler_params=pltpu.CompilerParams(vmem_limit_bytes=16 * 1024 * 1024),
        name="carry",
    )(place, everyone, earlier, scale, shift, out_weight)

    even, odd = (1, 0, 3, 2), (3, 2, 1, 0)

    def added(mine, came):
        return (mine.astype(jnp.float32) + came.astype(jnp.float32)).astype(jnp.bfloat16)

    def paired(value, by_core):
        pairs = [(2 * x + c, 2 * by_core[c][x] + c) for x in range(4) for c in range(2)]
        return lax.ppermute(value, TP, pairs)

    def summed(keep, send):
        mine = added(keep, swap_cores(send))
        mine = added(mine, paired(mine, (even, odd)))
        return mine, paired(mine, (odd, even))

    middle, near = pl.pallas_call(
        norm_body,
        out_shape=(half_shape, half_shape),
        in_specs=[smem] + [vmem] * 4,
        out_specs=(vmem, vmem),
        compiler_params=pltpu.CompilerParams(vmem_limit_bytes=16 * 1024 * 1024),
        name="norm",
    )(place, residual_in, *summed(keep, send), norm_gain.reshape(1, width))
    far = swap_cores(near)

    parts = 8
    last = 3 * units % wide + (units - 3 * units % wide) % wide
    send, keep = pl.pallas_call(
        feed_body,
        out_shape=(half_shape, half_shape),
        in_specs=[vmem, vmem, pl.BlockSpec(memory_space=pl.ANY)],
        out_specs=(vmem, vmem),
        scratch_shapes=[
            pltpu.VMEM((length, width), jnp.bfloat16),
            pltpu.VMEM((parts, count // parts, lot, wide), jnp.bfloat16),
            pltpu.VMEM((parts, width // parts, last), jnp.bfloat16),
            pltpu.VMEM((length, 2 * units), jnp.float32),
            pltpu.VMEM((length, units), jnp.bfloat16),
            pltpu.SemaphoreType.DMA((parts,)),
        ],
        compiler_params=pltpu.CompilerParams(vmem_limit_bytes=28 * 1024 * 1024),
        name="feed",
    )(
        pltpu.with_memory_space_constraint(near, pltpu.VMEM),
        pltpu.with_memory_space_constraint(far, pltpu.VMEM),
        pltpu.with_memory_space_constraint(weights, pltpu.HBM),
    )
    mine, came = summed(keep, send)
    channel_out = mine.astype(jnp.float32) + came.astype(jnp.float32)
    mine = (middle.astype(jnp.float32) + channel_out).astype(jnp.bfloat16)
    other = swap_cores(mine)
    first = jnp.where(core == 0, mine, other)
    last = jnp.where(core == 0, other, mine)
    return jnp.concatenate([first, last], axis=0)


def solution(mesh):
    sizes = (8, mesh.shape["sp"] // 8, mesh.shape["tp"] // 2, 2)
    torus = Mesh(mesh.devices.reshape(sizes), ("z", "y", "x", "core"))
    in_specs = (
        P(SP, None),
        P(TP, SP),
        P(TP, SP),
        P(TP, None),
        P(TP, None, None),
        P(TP, None, None),
        P(TP),
        P(TP, SP),
        P(TP, None),
        P(),
        P(SP, TP),
        P(SP, TP),
        P(SP, TP),
    )
    return jax.shard_map(
        on_device, mesh=torus, in_specs=in_specs, out_specs=P(SP, None), check_vma=False
    )
```

```python
import jax
import jax.numpy as jnp
from jax import lax
from jax.experimental import pallas as pl
from jax.experimental.pallas import tpu as pltpu
from jax.sharding import Mesh
from jax.sharding import PartitionSpec as P

SP = ("z", "y")
TP = ("x", "core")


def shifted(value, by, fill):
    rows = value.shape[0]
    head = jnp.full((by, value.shape[1]), fill, value.dtype)
    if by % 8 == 0:
        return jnp.concatenate([head, value[: rows - by]], axis=0)
    rolled = pltpu.roll(value, by, 0)
    row = lax.broadcasted_iota(jnp.int32, value.shape, 0)
    return jnp.where(row < by, jnp.asarray(fill, value.dtype), rolled)


def recurrence_body(
    mixer, before, taps, recur, admit, rate, extra, branch, scale_out, shift_out, ends_out
):
    channels, length = mixer.shape
    tap_count = taps.shape[1]
    signal = mixer[...].astype(jnp.float32).T
    eye = (
        lax.broadcasted_iota(jnp.int32, (channels, channels), 0)
        == lax.broadcasted_iota(jnp.int32, (channels, channels), 1)
    ).astype(jnp.bfloat16)
    turn = (((0,), (0,)), ((), ()))
    tap_rows = lax.dot_general(taps[...], eye, turn, preferred_element_type=jnp.float32)
    halo = lax.dot_general(before[...], eye, turn, preferred_element_type=jnp.float32)
    row = lax.broadcasted_iota(jnp.int32, signal.shape, 0)
    conv_sum = jnp.zeros(signal.shape, jnp.float32)
    for tap in range(tap_count):
        back = tap_count - 1 - tap
        moved = signal
        if back:
            moved = pltpu.roll(signal, back, 0)
            for line in range(back):
                moved = jnp.where(row == line, halo[tap + line : tap + line + 1], moved)
        conv_sum = conv_sum + tap_rows[tap : tap + 1] * moved
    conv_out = conv_sum.astype(jnp.bfloat16)
    groups, width, _ = recur.shape
    spread = (
        lax.broadcasted_iota(jnp.int32, (width, channels), 1) % width
        == lax.broadcasted_iota(jnp.int32, (width, channels), 0)
    ).astype(jnp.bfloat16)
    same = (
        lax.broadcasted_iota(jnp.int32, (channels, channels), 0) // width
        == lax.broadcasted_iota(jnp.int32, (channels, channels), 1) // width
    )

    def gate(weight):
        flat = weight[...].reshape(groups * width, width)
        wide = jnp.dot(flat, spread, preferred_element_type=jnp.float32)
        wide = jnp.where(same, wide, 0.0).astype(jnp.bfloat16)
        return jax.nn.sigmoid(jnp.dot(conv_out, wide, preferred_element_type=jnp.float32))

    recur_gate = gate(recur)
    admit_gate = gate(admit)
    log_decay = -8.0 * recur_gate * rate[...] + extra[...].T
    run = jnp.exp(log_decay)
    twice = 2.0 * log_decay
    series = twice * (1.0 + twice * (0.5 + twice * (1.0 / 6.0 + twice * (1.0 / 24.0 + twice * (
        1.0 / 120.0 + twice * (1.0 / 720.0))))))
    lost = -jnp.where(twice > -0.25, series, run * run - 1.0)
    kept = jnp.where(lost > 0.0, jnp.sqrt(lost), 0.0)
    state = kept * admit_gate * conv_out.astype(jnp.float32)
    by = 1
    while by < length:
        state = state + run * shifted(state, by, 0.0)
        run = run * shifted(run, by, 1.0)
        by *= 2
    ends_out[0:1] = run[length - 1 : length]
    ends_out[1:2] = state[length - 1 : length]
    gelu = jax.nn.gelu(branch[...].astype(jnp.float32), approximate=True).T
    scale_out[...] = run * gelu
    shift_out[...] = state * gelu


def folded(pairs, limit, scale, shift):
    for k in range(pairs.shape[0]):
        pair = pairs[k]
        after_scale, after_shift = pair[0:1] * scale, pair[0:1] * shift + pair[1:2]
        scale = jnp.where(k < limit, after_scale, scale)
        shift = jnp.where(k < limit, after_shift, shift)
    return scale, shift


def combine_body(place, line, before, total):
    one = jnp.ones((1, line.shape[2]), jnp.float32)
    for target, limit in ((before, place[0]), (total, line.shape[0])):
        scale, shift = folded(line, limit, one, 0.0 * one)
        target[0:1] = scale
        target[1:2] = shift


def carry_body(place, rows, before, scale, shift, weight, send, keep):
    core, z = place[1], place[2]
    half = send.shape[0]
    one = jnp.ones((1, scale.shape[1]), jnp.float32)
    entering = folded(rows, z, one, 0.0 * one)[1]
    entering = before[0:1] * entering + before[1:2]
    for target, side in ((send, 1 - core), (keep, core)):
        at = pl.ds(pl.multiple_of(side * half, half), half)
        mixed = (shift[at, :] + scale[at, :] * entering).astype(jnp.bfloat16)
        found = jnp.dot(mixed, weight[...], preferred_element_type=jnp.float32)
        target[...] = found.astype(jnp.bfloat16)


def norm_body(place, residual, mine, came, gain, middle, normed):
    half = middle.shape[0]
    branch = mine[...].astype(jnp.float32) + came[...].astype(jnp.float32)
    rows = pl.ds(pl.multiple_of(place[1] * half, half), half)
    found = (residual[rows, :].astype(jnp.float32) + branch).astype(jnp.bfloat16)
    middle[...] = found
    wide = found.astype(jnp.float32)
    row_scale = lax.rsqrt(jnp.mean(wide * wide, axis=1, keepdims=True) + 1e-06)
    normed[...] = (wide * row_scale * gain[...].astype(jnp.float32)).astype(jnp.bfloat16)


def pack_body(gate, up, down, out):
    rows, units = gate.shape
    wide = out.shape[1]
    blocks = 3 * units // wide
    spare = 3 * units - blocks * wide
    last = down[...].astype(jnp.float32)[:, units - spare :]
    parts = [down[...].astype(jnp.float32)[:, : units - spare]]
    parts += [gate[...].astype(jnp.float32), up[...].astype(jnp.float32)]
    joined = jnp.concatenate(parts, axis=1)
    for k in range(blocks):
        piece = joined[:, k * wide : (k + 1) * wide].astype(out.dtype)
        out[k * rows : (k + 1) * rows, :] = piece
    lines = rows * spare // wide
    lot = [last[k * lines : (k + 1) * lines] for k in range(rows // lines)]
    out[blocks * rows :, :] = jnp.concatenate(lot, axis=1).astype(out.dtype)


def feed_body(near, far, weights, send, keep, rows, stage, tail, both_sum, hidden, arrived):
    parts, group, lot, wide = stage.shape
    half = near.shape[0]
    units = hidden.shape[1]
    blocks = 3 * units // wide
    share = rows.shape[1] // (parts * group)
    span = group * share
    spare = 3 * units - blocks * wide
    full = (units - spare) // wide
    begin = units - spare - full * wide
    copies = [
        pltpu.make_async_copy(weights.at[pl.ds(k * group, group)], stage.at[k], arrived.at[k])
        for k in range(parts)
    ]
    for copy in copies:
        copy.start()
    rows[:half] = near[...]
    rows[half:] = far[...]

    def block(k, at):
        return stage[k, :, at * share : (at + 1) * share, :].reshape(span, wide)

    for k in range(0, parts, 2):
        for piece in (k, k + 1):
            copies[piece].wait()
            loose = stage[piece, :, blocks * share :, :].astype(jnp.float32)
            loose = [loose[:, :, at * spare : (at + 1) * spare] for at in range(wide // spare)]
            loose = jnp.concatenate(loose, axis=1).astype(tail.dtype).reshape(span, spare)
            tail[piece, :, :begin] = block(piece, full)[:, :begin]
            tail[piece, :, begin:] = loose
        for at in range(full, blocks):
            start = begin if at == full else 0
            found = None
            for piece in (k, k + 1):
                weight = block(piece, at)[:, start:]
                mine = rows[:, piece * span : (piece + 1) * span]
                part = jnp.dot(mine, weight, preferred_element_type=jnp.float32)
                found = part if found is None else found + part
            first = at * wide + start - (units - spare)
            columns = slice(first, first + wide - start)
            if k == 0:
                both_sum[:, columns] = found
            else:
                both_sum[:, columns] += found
    gated = both_sum[:, :units]
    silu = gated / (1.0 + jnp.exp(-gated))
    hidden[...] = (silu * both_sum[:, units:]).astype(jnp.bfloat16)
    flip = (((1,), (1,)), ((), ()))
    for k in range(parts):
        found = lax.dot_general(
            hidden[:, full * wide :], tail[k], flip, preferred_element_type=jnp.float32
        )
        for at in range(full):
            piece = hidden[:, at * wide : (at + 1) * wide]
            found = found + lax.dot_general(
                piece, block(k, at), flip, preferred_element_type=jnp.float32
            )
        keep[:, k * span : (k + 1) * span] = found[:half].astype(jnp.bfloat16)
        send[:, k * span : (k + 1) * span] = found[half:].astype(jnp.bfloat16)


def sent_to_all(value, axis):
    count = lax.axis_size(axis)
    return lax.all_to_all(
        jnp.broadcast_to(value[None], (count, *value.shape)), axis, 0, 0, tiled=True
    )


def swap_cores(value):
    return lax.ppermute(value, "core", [(0, 1), (1, 0)])


def on_device(
    residual_in,
    mixer_input,
    branch_gate,
    conv_taps,
    recur_weight,
    admit_weight,
    decay_param,
    decay_extra,
    out_weight,
    norm_gain,
    gate_weight,
    up_weight,
    down_weight,
):
    shard, units = gate_weight.shape
    wide = 256
    lot = 3 * units * shard // wide
    weights = pl.pallas_call(
        pack_body,
        out_shape=jax.ShapeDtypeStruct((lot, wide), gate_weight.dtype),
        compiler_params=pltpu.CompilerParams(vmem_limit_bytes=8 * 1024 * 1024),
        name="pack",
    )(*(pltpu.with_memory_space_constraint(w, pltpu.HBM) for w in (gate_weight, up_weight, down_weight)))
    weights = lax.all_gather(weights, SP, axis=0)

    channels, length = mixer_input.shape
    tap_count = conv_taps.shape[1]
    count = lax.axis_size(SP)
    tail = mixer_input[:, length - (tap_count - 1) :]
    before = lax.ppermute(tail, SP, [(i, i + 1) for i in range(count - 1)])
    square = jax.ShapeDtypeStruct((length, channels), jnp.float32)
    scale, shift, ends = pl.pallas_call(
        recurrence_body,
        out_shape=(square, square, jax.ShapeDtypeStruct((2, channels), jnp.float32)),
        in_specs=[pl.BlockSpec(memory_space=pltpu.VMEM)] * 8,
        out_specs=(pl.BlockSpec(memory_space=pltpu.VMEM),) * 3,
        compiler_params=pltpu.CompilerParams(vmem_limit_bytes=16 * 1024 * 1024),
        name="recurrence",
    )(
        mixer_input,
        before,
        conv_taps,
        recur_weight,
        admit_weight,
        jax.nn.softplus(-decay_param).reshape(1, channels),
        decay_extra,
        branch_gate,
    )
    smem = pl.BlockSpec(memory_space=pltpu.SMEM)
    vmem = pl.BlockSpec(memory_space=pltpu.VMEM)
    y_place = lax.axis_index("y").astype(jnp.int32).reshape(1)
    pair_shape = jax.ShapeDtypeStruct(ends.shape, jnp.float32)
    earlier, total = pl.pallas_call(
        combine_body,
        out_shape=(pair_shape, pair_shape),
        in_specs=[smem, vmem],
        out_specs=(vmem, vmem),
        compiler_params=pltpu.CompilerParams(vmem_limit_bytes=8 * 1024 * 1024),
        name="combine",
    )(y_place, sent_to_all(ends, "y"))
    everyone = sent_to_all(total, "z")
    core = lax.axis_index("core")
    place = jnp.stack([lax.axis_index(SP), core, lax.axis_index("z")]).astype(jnp.int32)
    half = length // 2
    width = out_weight.shape[1]
    half_shape = jax.ShapeDtypeStruct((half, width), jnp.bfloat16)
    send, keep = pl.pallas_call(
        carry_body,
        out_shape=(half_shape, half_shape),
        in_specs=[smem] + [vmem] * 5,
        out_specs=(vmem, vmem),
        compiler_params=pltpu.CompilerParams(vmem_limit_bytes=16 * 1024 * 1024),
        name="carry",
    )(place, everyone, earlier, scale, shift, out_weight)

    even, odd = (1, 0, 3, 2), (3, 2, 1, 0)

    def added(mine, came):
        return (mine.astype(jnp.float32) + came.astype(jnp.float32)).astype(jnp.bfloat16)

    def paired(value, by_core):
        pairs = [(2 * x + c, 2 * by_core[c][x] + c) for x in range(4) for c in range(2)]
        return lax.ppermute(value, TP, pairs)

    def summed(keep, send):
        mine = added(keep, swap_cores(send))
        mine = added(mine, paired(mine, (even, odd)))
        return mine, paired(mine, (odd, even))

    middle, near = pl.pallas_call(
        norm_body,
        out_shape=(half_shape, half_shape),
        in_specs=[smem] + [vmem] * 4,
        out_specs=(vmem, vmem),
        compiler_params=pltpu.CompilerParams(vmem_limit_bytes=16 * 1024 * 1024),
        name="norm",
    )(place, residual_in, *summed(keep, send), norm_gain.reshape(1, width))
    far = swap_cores(near)
    out, far = lax.optimization_barrier((residual_in, far))

    parts = 8
    last = 3 * units % wide + (units - 3 * units % wide) % wide
    send, keep = pl.pallas_call(
        feed_body,
        out_shape=(half_shape, half_shape),
        in_specs=[vmem, vmem, pl.BlockSpec(memory_space=pl.ANY)],
        out_specs=(vmem, vmem),
        scratch_shapes=[
            pltpu.VMEM((length, width), jnp.bfloat16),
            pltpu.VMEM((parts, count // parts, lot, wide), jnp.bfloat16),
            pltpu.VMEM((parts, width // parts, last), jnp.bfloat16),
            pltpu.VMEM((length, 2 * units), jnp.float32),
            pltpu.VMEM((length, units), jnp.bfloat16),
            pltpu.SemaphoreType.DMA((parts,)),
        ],
        compiler_params=pltpu.CompilerParams(vmem_limit_bytes=28 * 1024 * 1024),
        name="feed",
    )(
        pltpu.with_memory_space_constraint(near, pltpu.VMEM),
        pltpu.with_memory_space_constraint(far, pltpu.VMEM),
        pltpu.with_memory_space_constraint(weights, pltpu.HBM),
    )
    mine, came = summed(keep, send)
    channel_out = mine.astype(jnp.float32) + came.astype(jnp.float32)
    mine = (middle.astype(jnp.float32) + channel_out).astype(jnp.bfloat16)
    other = swap_cores(mine)
    for side, rows in ((core, mine), (1 - core, other)):
        out = lax.dynamic_update_slice_in_dim(out, rows, side * half, 0)
    return out


def solution(mesh):
    sizes = (8, mesh.shape["sp"] // 8, mesh.shape["tp"] // 2, 2)
    torus = Mesh(mesh.devices.reshape(sizes), ("z", "y", "x", "core"))
    in_specs = (
        P(SP, None),
        P(TP, SP),
        P(TP, SP),
        P(TP, None),
        P(TP, None, None),
        P(TP, None, None),
        P(TP),
        P(TP, SP),
        P(TP, None),
        P(),
        P(SP, TP),
        P(SP, TP),
        P(SP, TP),
    )
    return jax.shard_map(
        on_device, mesh=torus, in_specs=in_specs, out_specs=P(SP, None), check_vma=False
    )
```

```python
import jax
import jax.numpy as jnp
from jax import lax
from jax.experimental import pallas as pl
from jax.experimental.pallas import tpu as pltpu
from jax.sharding import Mesh
from jax.sharding import PartitionSpec as P

SP = ("z", "y")
TP = ("x", "core")


def shifted(value, by, fill):
    rows = value.shape[0]
    head = jnp.full((by, value.shape[1]), fill, value.dtype)
    if by % 8 == 0:
        return jnp.concatenate([head, value[: rows - by]], axis=0)
    rolled = pltpu.roll(value, by, 0)
    row = lax.broadcasted_iota(jnp.int32, value.shape, 0)
    return jnp.where(row < by, jnp.asarray(fill, value.dtype), rolled)


def recurrence_body(
    mixer, before, taps, recur, admit, rate, extra, branch, scale_out, shift_out, ends_out
):
    channels, length = mixer.shape
    tap_count = taps.shape[1]
    signal = mixer[...].astype(jnp.float32).T
    eye = (
        lax.broadcasted_iota(jnp.int32, (channels, channels), 0)
        == lax.broadcasted_iota(jnp.int32, (channels, channels), 1)
    ).astype(jnp.bfloat16)
    turn = (((0,), (0,)), ((), ()))
    tap_rows = lax.dot_general(taps[...], eye, turn, preferred_element_type=jnp.float32)
    halo = lax.dot_general(before[...], eye, turn, preferred_element_type=jnp.float32)
    row = lax.broadcasted_iota(jnp.int32, signal.shape, 0)
    conv_sum = jnp.zeros(signal.shape, jnp.float32)
    for tap in range(tap_count):
        back = tap_count - 1 - tap
        moved = signal
        if back:
            moved = pltpu.roll(signal, back, 0)
            for line in range(back):
                moved = jnp.where(row == line, halo[tap + line : tap + line + 1], moved)
        conv_sum = conv_sum + tap_rows[tap : tap + 1] * moved
    conv_out = conv_sum.astype(jnp.bfloat16)
    groups, width, _ = recur.shape
    spread = (
        lax.broadcasted_iota(jnp.int32, (width, channels), 1) % width
        == lax.broadcasted_iota(jnp.int32, (width, channels), 0)
    ).astype(jnp.bfloat16)
    same = (
        lax.broadcasted_iota(jnp.int32, (channels, channels), 0) // width
        == lax.broadcasted_iota(jnp.int32, (channels, channels), 1) // width
    )

    def gate(weight):
        flat = weight[...].reshape(groups * width, width)
        wide = jnp.dot(flat, spread, preferred_element_type=jnp.float32)
        wide = jnp.where(same, wide, 0.0).astype(jnp.bfloat16)
        return jax.nn.sigmoid(jnp.dot(conv_out, wide, preferred_element_type=jnp.float32))

    recur_gate = gate(recur)
    admit_gate = gate(admit)
    log_decay = -8.0 * recur_gate * rate[...] + extra[...].T
    run = jnp.exp(log_decay)
    twice = 2.0 * log_decay
    series = twice * (1.0 + twice * (0.5 + twice * (1.0 / 6.0 + twice * (1.0 / 24.0 + twice * (
        1.0 / 120.0 + twice * (1.0 / 720.0))))))
    lost = -jnp.where(twice > -0.25, series, run * run - 1.0)
    kept = jnp.where(lost > 0.0, jnp.sqrt(lost), 0.0)
    state = kept * admit_gate * conv_out.astype(jnp.float32)
    by = 1
    while by < length:
        state = state + run * shifted(state, by, 0.0)
        run = run * shifted(run, by, 1.0)
        by *= 2
    ends_out[0:1] = run[length - 1 : length]
    ends_out[1:2] = state[length - 1 : length]
    gelu = jax.nn.gelu(branch[...].astype(jnp.float32), approximate=True).T
    scale_out[...] = run * gelu
    shift_out[...] = state * gelu


def folded(pairs, limit, scale, shift):
    for k in range(pairs.shape[0]):
        pair = pairs[k]
        after_scale, after_shift = pair[0:1] * scale, pair[0:1] * shift + pair[1:2]
        scale = jnp.where(k < limit, after_scale, scale)
        shift = jnp.where(k < limit, after_shift, shift)
    return scale, shift


def combine_body(place, line, before, total):
    one = jnp.ones((1, line.shape[2]), jnp.float32)
    for target, limit in ((before, place[0]), (total, line.shape[0])):
        scale, shift = folded(line, limit, one, 0.0 * one)
        target[0:1] = scale
        target[1:2] = shift


def carry_body(place, rows, before, scale, shift, weight, send, keep):
    core, z = place[1], place[2]
    half = send.shape[0]
    one = jnp.ones((1, scale.shape[1]), jnp.float32)
    entering = folded(rows, z, one, 0.0 * one)[1]
    entering = before[0:1] * entering + before[1:2]
    for target, side in ((send, 1 - core), (keep, core)):
        at = pl.ds(pl.multiple_of(side * half, half), half)
        mixed = (shift[at, :] + scale[at, :] * entering).astype(jnp.bfloat16)
        found = jnp.dot(mixed, weight[...], preferred_element_type=jnp.float32)
        target[...] = found.astype(jnp.bfloat16)


def norm_body(place, residual, mine, came, gain, middle, normed):
    half = middle.shape[0]
    branch = mine[...].astype(jnp.float32) + came[...].astype(jnp.float32)
    rows = pl.ds(pl.multiple_of(place[1] * half, half), half)
    found = (residual[rows, :].astype(jnp.float32) + branch).astype(jnp.bfloat16)
    middle[...] = found
    wide = found.astype(jnp.float32)
    row_scale = lax.rsqrt(jnp.mean(wide * wide, axis=1, keepdims=True) + 1e-06)
    normed[...] = (wide * row_scale * gain[...].astype(jnp.float32)).astype(jnp.bfloat16)


def pack_body(gate, up, down, out):
    rows, units = gate.shape
    wide = out.shape[1]
    blocks = 3 * units // wide
    spare = 3 * units - blocks * wide
    last = down[...].astype(jnp.float32)[:, units - spare :]
    parts = [down[...].astype(jnp.float32)[:, : units - spare]]
    parts += [gate[...].astype(jnp.float32), up[...].astype(jnp.float32)]
    joined = jnp.concatenate(parts, axis=1)
    for k in range(blocks):
        piece = joined[:, k * wide : (k + 1) * wide].astype(out.dtype)
        out[k * rows : (k + 1) * rows, :] = piece
    lines = rows * spare // wide
    lot = [last[k * lines : (k + 1) * lines] for k in range(rows // lines)]
    out[blocks * rows :, :] = jnp.concatenate(lot, axis=1).astype(out.dtype)


def feed_body(near, far, weights, send, keep, rows, stage, tail, both_sum, hidden, arrived):
    parts, group, lot, wide = stage.shape
    half = near.shape[0]
    units = hidden.shape[1]
    blocks = 3 * units // wide
    share = rows.shape[1] // (parts * group)
    span = group * share
    spare = 3 * units - blocks * wide
    full = (units - spare) // wide
    begin = units - spare - full * wide
    copies = [
        pltpu.make_async_copy(weights.at[pl.ds(k * group, group)], stage.at[k], arrived.at[k])
        for k in range(parts)
    ]
    for copy in copies:
        copy.start()
    rows[:half] = near[...]
    rows[half:] = far[...]

    def block(k, at):
        return stage[k, :, at * share : (at + 1) * share, :].reshape(span, wide)

    groups, k = [], 0
    for size in (2, 3, 2, 1):
        groups.append(range(k, k + size))
        k += size
    for pieces in groups:
        for piece in pieces:
            copies[piece].wait()
            loose = stage[piece, :, blocks * share :, :].astype(jnp.float32)
            loose = [loose[:, :, at * spare : (at + 1) * spare] for at in range(wide // spare)]
            loose = jnp.concatenate(loose, axis=1).astype(tail.dtype).reshape(span, spare)
            tail[piece, :, :begin] = block(piece, full)[:, :begin]
            tail[piece, :, begin:] = loose
        for at in range(full, blocks):
            start = begin if at == full else 0
            found = None
            for piece in pieces:
                weight = block(piece, at)[:, start:]
                mine = rows[:, piece * span : (piece + 1) * span]
                part = jnp.dot(mine, weight, preferred_element_type=jnp.float32)
                found = part if found is None else found + part
            first = at * wide + start - (units - spare)
            columns = slice(first, first + wide - start)
            if pieces[0] == 0:
                both_sum[:, columns] = found
            else:
                both_sum[:, columns] += found
    gated = both_sum[:, :units]
    silu = gated / (1.0 + jnp.exp(-gated))
    hidden[...] = (silu * both_sum[:, units:]).astype(jnp.bfloat16)
    flip = (((1,), (1,)), ((), ()))
    for k in range(parts):
        found = lax.dot_general(
            hidden[:, full * wide :], tail[k], flip, preferred_element_type=jnp.float32
        )
        for at in range(full):
            piece = hidden[:, at * wide : (at + 1) * wide]
            found = found + lax.dot_general(
                piece, block(k, at), flip, preferred_element_type=jnp.float32
            )
        keep[:, k * span : (k + 1) * span] = found[:half].astype(jnp.bfloat16)
        send[:, k * span : (k + 1) * span] = found[half:].astype(jnp.bfloat16)


def sent_to_all(value, axis):
    count = lax.axis_size(axis)
    return lax.all_to_all(
        jnp.broadcast_to(value[None], (count, *value.shape)), axis, 0, 0, tiled=True
    )


def swap_cores(value):
    return lax.ppermute(value, "core", [(0, 1), (1, 0)])


def on_device(
    residual_in,
    mixer_input,
    branch_gate,
    conv_taps,
    recur_weight,
    admit_weight,
    decay_param,
    decay_extra,
    out_weight,
    norm_gain,
    gate_weight,
    up_weight,
    down_weight,
):
    shard, units = gate_weight.shape
    wide = 256
    lot = 3 * units * shard // wide
    weights = pl.pallas_call(
        pack_body,
        out_shape=jax.ShapeDtypeStruct((lot, wide), gate_weight.dtype),
        compiler_params=pltpu.CompilerParams(vmem_limit_bytes=8 * 1024 * 1024),
        name="pack",
    )(*(pltpu.with_memory_space_constraint(w, pltpu.HBM) for w in (gate_weight, up_weight, down_weight)))
    weights = lax.all_gather(weights, SP, axis=0)

    channels, length = mixer_input.shape
    tap_count = conv_taps.shape[1]
    count = lax.axis_size(SP)
    tail = mixer_input[:, length - (tap_count - 1) :]
    before = lax.ppermute(tail, SP, [(i, i + 1) for i in range(count - 1)])
    square = jax.ShapeDtypeStruct((length, channels), jnp.float32)
    scale, shift, ends = pl.pallas_call(
        recurrence_body,
        out_shape=(square, square, jax.ShapeDtypeStruct((2, channels), jnp.float32)),
        in_specs=[pl.BlockSpec(memory_space=pltpu.VMEM)] * 8,
        out_specs=(pl.BlockSpec(memory_space=pltpu.VMEM),) * 3,
        compiler_params=pltpu.CompilerParams(vmem_limit_bytes=16 * 1024 * 1024),
        name="recurrence",
    )(
        mixer_input,
        before,
        conv_taps,
        recur_weight,
        admit_weight,
        jax.nn.softplus(-decay_param).reshape(1, channels),
        decay_extra,
        branch_gate,
    )
    smem = pl.BlockSpec(memory_space=pltpu.SMEM)
    vmem = pl.BlockSpec(memory_space=pltpu.VMEM)
    y_place = lax.axis_index("y").astype(jnp.int32).reshape(1)
    pair_shape = jax.ShapeDtypeStruct(ends.shape, jnp.float32)
    earlier, total = pl.pallas_call(
        combine_body,
        out_shape=(pair_shape, pair_shape),
        in_specs=[smem, vmem],
        out_specs=(vmem, vmem),
        compiler_params=pltpu.CompilerParams(vmem_limit_bytes=8 * 1024 * 1024),
        name="combine",
    )(y_place, sent_to_all(ends, "y"))
    everyone = sent_to_all(total, "z")
    core = lax.axis_index("core")
    place = jnp.stack([lax.axis_index(SP), core, lax.axis_index("z")]).astype(jnp.int32)
    half = length // 2
    width = out_weight.shape[1]
    half_shape = jax.ShapeDtypeStruct((half, width), jnp.bfloat16)
    send, keep = pl.pallas_call(
        carry_body,
        out_shape=(half_shape, half_shape),
        in_specs=[smem] + [vmem] * 5,
        out_specs=(vmem, vmem),
        compiler_params=pltpu.CompilerParams(vmem_limit_bytes=16 * 1024 * 1024),
        name="carry",
    )(place, everyone, earlier, scale, shift, out_weight)

    even, odd = (1, 0, 3, 2), (3, 2, 1, 0)

    def added(mine, came):
        return (mine.astype(jnp.float32) + came.astype(jnp.float32)).astype(jnp.bfloat16)

    def paired(value, by_core):
        pairs = [(2 * x + c, 2 * by_core[c][x] + c) for x in range(4) for c in range(2)]
        return lax.ppermute(value, TP, pairs)

    def summed(keep, send):
        mine = added(keep, swap_cores(send))
        mine = added(mine, paired(mine, (even, odd)))
        return mine, paired(mine, (odd, even))

    middle, near = pl.pallas_call(
        norm_body,
        out_shape=(half_shape, half_shape),
        in_specs=[smem] + [vmem] * 4,
        out_specs=(vmem, vmem),
        compiler_params=pltpu.CompilerParams(vmem_limit_bytes=16 * 1024 * 1024),
        name="norm",
    )(place, residual_in, *summed(keep, send), norm_gain.reshape(1, width))
    far = swap_cores(near)
    out, far = lax.optimization_barrier((residual_in, far))

    parts = 8
    last = 3 * units % wide + (units - 3 * units % wide) % wide
    send, keep = pl.pallas_call(
        feed_body,
        out_shape=(half_shape, half_shape),
        in_specs=[vmem, vmem, pl.BlockSpec(memory_space=pl.ANY)],
        out_specs=(vmem, vmem),
        scratch_shapes=[
            pltpu.VMEM((length, width), jnp.bfloat16),
            pltpu.VMEM((parts, count // parts, lot, wide), jnp.bfloat16),
            pltpu.VMEM((parts, width // parts, last), jnp.bfloat16),
            pltpu.VMEM((length, 2 * units), jnp.float32),
            pltpu.VMEM((length, units), jnp.bfloat16),
            pltpu.SemaphoreType.DMA((parts,)),
        ],
        compiler_params=pltpu.CompilerParams(vmem_limit_bytes=28 * 1024 * 1024),
        name="feed",
    )(
        pltpu.with_memory_space_constraint(near, pltpu.VMEM),
        pltpu.with_memory_space_constraint(far, pltpu.VMEM),
        pltpu.with_memory_space_constraint(weights, pltpu.HBM),
    )
    mine, came = summed(keep, send)
    channel_out = mine.astype(jnp.float32) + came.astype(jnp.float32)
    mine = (middle.astype(jnp.float32) + channel_out).astype(jnp.bfloat16)
    other = swap_cores(mine)
    for side, rows in ((core, mine), (1 - core, other)):
        out = lax.dynamic_update_slice_in_dim(out, rows, side * half, 0)
    return out


def solution(mesh):
    sizes = (8, mesh.shape["sp"] // 8, mesh.shape["tp"] // 2, 2)
    torus = Mesh(mesh.devices.reshape(sizes), ("z", "y", "x", "core"))
    in_specs = (
        P(SP, None),
        P(TP, SP),
        P(TP, SP),
        P(TP, None),
        P(TP, None, None),
        P(TP, None, None),
        P(TP),
        P(TP, SP),
        P(TP, None),
        P(),
        P(SP, TP),
        P(SP, TP),
        P(SP, TP),
    )
    return jax.shard_map(
        on_device, mesh=torus, in_specs=in_specs, out_specs=P(SP, None), check_vma=False
    )
```
